32 devices in a mesh: rep: 4 (over z), fs: 4 (over y, x), tp: 2 (over core).
Axes of the slice: x: 2, y: 2, z: 4, core: 2. Of those that a mesh axis runs over, the one named last changes fastest.
Arguments:
- tokens: bfloat16 [2048, 1024], P(('rep', 'fs', 'tp')), may hold values from -6 to 6
- cotangent: bfloat16 [2048, 1024], P(('rep', 'fs', 'tp')), may hold values from -6 to 6
- gate_weight: bfloat16 [1024, 2816], P('fs', 'tp'), may hold values from -0.1875 to 0.1875
- up_weight: bfloat16 [1024, 2816], P('fs', 'tp'), may hold values from -0.1875 to 0.1875
- down_weight: bfloat16 [2816, 1024], P('tp', 'fs'), may hold values from -0.109375 to 0.109375
Outputs:
- input_grad: bfloat16 [2048, 1024], P(('rep', 'fs', 'tp'))
- gate_grad: float32 [1024, 2816], P('fs', 'tp')
- up_grad: float32 [1024, 2816], P('fs', 'tp')
- down_grad: float32 [2816, 1024], P('tp', 'fs')
- gate_power: float32 [1024], P('fs')
- up_power: float32 [1024], P('fs')
- down_power: float32 [2816], P('tp')
The draws below stay inside these ranges and needn't reach their ends.
All inputs are finite; a program needn't handle non-finite values.
Results may differ from the reference program's by a relative error of at most 0.0017.
Values may be sent and summed in bfloat16 or wider, within the bound.
A program may use at most 64 MiB of HBM per device.

```python
import jax
import jax.numpy as jnp
from jax import lax

D = 1024
FF = 2816
TOKENS = 2048
N_REP = 4
N_FS = 4


def spiked(result, rng, source, target, parts, factor):
    def block_of(position):
        return (jnp.arange(result.shape[position]) // (result.shape[position] // parts)).reshape((-1,) + (1,) * (result.ndim - 1 - position))

    near = jax.random.permutation(rng, parts)[block_of(target)]
    far = (block_of(target) + parts // 2) % parts
    return jnp.where((block_of(source) == near) | (block_of(source) == far), factor * result, result)


def block_scale(rng, shape, cuts, least, high):
    loudness, own = 1.0, jax.random.fold_in(rng, 6)
    for axis_at, blocks in cuts:
        steps = jnp.exp(jax.random.uniform(jax.random.fold_in(own, axis_at), (blocks,), jnp.float32, least / len(cuts), high / len(cuts)))
        loudness = loudness * jnp.repeat(steps, shape[axis_at] // blocks).reshape([-1 if axis == axis_at else 1 for axis in range(len(shape))])
    return loudness


def bell_draw(rng, dims, spread, limit, cuts=(), dtype=jnp.bfloat16):
    values = spread * jax.random.normal(rng, dims, jnp.float32)
    if cuts:
        values = values * block_scale(rng, dims, cuts, -0.22, 0.18)
    return jnp.clip(values, -limit, limit).astype(dtype)


def bell_draw_with(rng, extent, scale, limit, cuts, heavy, held_as=jnp.bfloat16):
    values = scale * jax.random.normal(rng, extent, jnp.float32)
    if cuts:
        values = values * block_scale(rng, extent, cuts, -0.22, 0.18)
    return jnp.clip(spiked(values, jax.random.fold_in(rng, 3), *heavy), -limit, limit).astype(held_as)


def setup_inputs(seed: int = 0) -> dict:
    arg_keys = jax.random.split(jax.random.key(seed), 6)
    tokens = bell_draw(arg_keys[0], (TOKENS, D), 1.0, 6.0, ((0, 32),))
    cotangent = bell_draw_with(arg_keys[1], (TOKENS, D), 1.0, 6.0, ((0, 32),), (0, 1, 32, 2.75))
    gate_weight = bell_draw(arg_keys[2], (D, FF), D ** -0.5, 0.1875, ((0, 4), (1, 2)))
    up_weight = bell_draw(arg_keys[3], (D, FF), D ** -0.5, 0.1875, ((0, 4), (1, 2)))
    down_weight = bell_draw(arg_keys[4], (FF, D), FF ** -0.5, 0.109375, ((0, 2), (1, 4)))
    return dict(tokens=tokens, cotangent=cotangent, gate_weight=gate_weight, up_weight=up_weight, down_weight=down_weight)


EPSILON = 1e-06

def contract_rows(left, right):
    return lax.dot_general(left, right, (((0,), (0,)), ((), ())), preferred_element_type=jnp.float32)

def contract_cols(left, right):
    return lax.dot_general(left, right, (((1,), (1,)), ((), ())), preferred_element_type=jnp.float32)

def local_pass(tokens, cotangent, gate_weight, up_weight, down_cols):
    xfloat = tokens.astype(jnp.float32)
    recip_norm = lax.rsqrt(lax.optimization_barrier(jnp.mean(xfloat * xfloat, axis=1, keepdims=True)) + EPSILON)
    normed_exact = xfloat * recip_norm
    normed = normed_exact.astype(jnp.bfloat16)
    gate_pre = jnp.dot(normed, gate_weight, preferred_element_type=jnp.float32)
    up_pre = jnp.dot(normed, up_weight, preferred_element_type=jnp.float32)
    sigmoid_gate = jax.nn.sigmoid(gate_pre)
    activated = gate_pre * sigmoid_gate
    hidden = (activated * up_pre).astype(jnp.bfloat16)
    grad_hidden = 0.5 * jnp.dot(cotangent, down_cols, preferred_element_type=jnp.float32)
    grad_up_pre = (grad_hidden * activated).astype(jnp.bfloat16)
    grad_gate_pre = (grad_hidden * up_pre * sigmoid_gate * (1.0 + gate_pre * (1.0 - sigmoid_gate))).astype(jnp.bfloat16)
    grad_normed = contract_cols(grad_gate_pre, gate_weight) + contract_cols(grad_up_pre, up_weight)
    terms = (contract_rows(normed, grad_gate_pre), contract_rows(normed, grad_up_pre), 0.5 * contract_rows(cotangent, hidden))
    return (normed_exact, recip_norm, grad_normed, terms)

def finish_input(normed_exact, recip_norm, grad_normed):
    inner = lax.optimization_barrier(jnp.mean(grad_normed * normed_exact, axis=1, keepdims=True))
    return (recip_norm * (grad_normed - normed_exact * inner)).astype(jnp.bfloat16)

def reference(tokens, cotangent, gate_weight, up_weight, down_weight):
    blocks = N_REP * N_FS
    down_cols = down_weight.T
    token_blocks = tokens.reshape(blocks, -1, D)
    cotangent_blocks = cotangent.reshape(blocks, -1, D)
    zeros = jnp.zeros((D, FF), jnp.float32)

    def block_step(carry, pieces):
        normed_exact, recip_norm, grad_normed, terms = local_pass(pieces[0], pieces[1], gate_weight, up_weight, down_cols)
        carry = (carry[0] + terms[0], carry[1] + terms[1], carry[2] + terms[2])
        return (carry, finish_input(normed_exact, recip_norm, grad_normed))
    totals, input_blocks = lax.scan(block_step, (zeros, zeros, zeros), (token_blocks, cotangent_blocks))
    factor = 1.0 / float(TOKENS) ** 0.5
    gate_grad = totals[0] * factor
    up_grad = totals[1] * factor
    down_grad = (totals[2] * factor).T
    gate_power = lax.optimization_barrier(jnp.sum(gate_grad * gate_grad, axis=1)) / FF
    up_power = lax.optimization_barrier(jnp.sum(up_grad * up_grad, axis=1)) / FF
    down_power = lax.optimization_barrier(jnp.sum(down_grad * down_grad, axis=1)) / D
    return (input_blocks.reshape(TOKENS, D), gate_grad, up_grad, down_grad, gate_power, up_power, down_power)
```

```python
import functools
import math

import jax
import jax.numpy as jnp
from jax import lax
from jax.experimental import pallas as pl
from jax.experimental.pallas import tpu as pltpu
from jax.sharding import PartitionSpec as P

D = 1024
FF = 2816


EPSILON = 1e-06


def contract_rows(left, right):
    return lax.dot_general(
        left, right, (((0,), (0,)), ((), ())), preferred_element_type=jnp.float32
    )


def contract_cols(left, right):
    return lax.dot_general(
        left, right, (((1,), (1,)), ((), ())), preferred_element_type=jnp.float32
    )


def on_device(tokens, cotangent, gate_weight, up_weight, down_weight):
    tp_count = lax.axis_size("tp")
    fs_count = lax.axis_size("fs")
    rep_count = lax.axis_size("rep")
    width = tokens.shape[1]
    factor = 1.0 / math.sqrt(tokens.shape[0] * tp_count * fs_count * rep_count)
    xfloat = tokens.astype(jnp.float32)
    recip_norm = lax.rsqrt(jnp.mean(xfloat * xfloat, axis=1, keepdims=True) + EPSILON)
    normed_exact = xfloat * recip_norm
    normed = normed_exact.astype(jnp.bfloat16)
    group_normed, group_cotangent = (
        lax.all_gather(normed, "tp", axis=0, tiled=True),
        lax.all_gather(cotangent, "tp", axis=0, tiled=True),
    )
    gate_full, up_full, down_full = (
        lax.all_gather(gate_weight, "fs", axis=0, tiled=True),
        lax.all_gather(up_weight, "fs", axis=0, tiled=True),
        lax.all_gather(down_weight.T, "fs", axis=0, tiled=True),
    )
    gate_pre = jnp.dot(group_normed, gate_full, preferred_element_type=jnp.float32)
    up_pre = jnp.dot(group_normed, up_full, preferred_element_type=jnp.float32)
    sigmoid_gate = jax.nn.sigmoid(gate_pre)
    activated = gate_pre * sigmoid_gate
    hidden = (activated * up_pre).astype(jnp.bfloat16)
    grad_hidden = 0.5 * jnp.dot(group_cotangent, down_full, preferred_element_type=jnp.float32)
    grad_up_pre = (grad_hidden * activated).astype(jnp.bfloat16)
    grad_gate_pre = (
        grad_hidden * up_pre * sigmoid_gate * (1.0 + gate_pre * (1.0 - sigmoid_gate))
    ).astype(jnp.bfloat16)
    normed_part = contract_cols(grad_gate_pre, gate_full) + contract_cols(grad_up_pre, up_full)
    grad_normed = lax.psum_scatter(normed_part, "tp", scatter_dimension=0, tiled=True)
    inner = jnp.mean(grad_normed * normed_exact, axis=1, keepdims=True)
    input_grad = (recip_norm * (grad_normed - normed_exact * inner)).astype(jnp.bfloat16)
    hidden_local = gate_weight.shape[1]

    def rows_term():
        normed_cols = lax.slice_in_dim(
            group_normed, 0, width // fs_count * lax.axis_size("fs"), axis=1
        )
        cotangent_cols = lax.slice_in_dim(
            group_cotangent, 0, width // fs_count * lax.axis_size("fs"), axis=1
        )
        return factor * jnp.concatenate(
            [
                contract_rows(normed_cols, grad_gate_pre),
                contract_rows(normed_cols, grad_up_pre),
                0.5 * contract_rows(cotangent_cols, hidden),
            ],
            axis=1,
        )

    reduced = lax.psum_scatter(rows_term(), "fs", scatter_dimension=0, tiled=True)
    reduced = lax.psum(reduced, "rep")
    gate_grad = reduced[:, :hidden_local]
    up_grad = reduced[:, hidden_local : 2 * hidden_local]
    down_grad = reduced[:, 2 * hidden_local :].T
    gate_sums, up_sums = lax.psum(
        (jnp.sum(gate_grad * gate_grad, axis=1), jnp.sum(up_grad * up_grad, axis=1)), "tp"
    )
    down_sums = lax.psum(jnp.sum(down_grad * down_grad, axis=1), "fs")
    return (input_grad, gate_grad, up_grad, down_grad, gate_sums / FF, up_sums / FF, down_sums / D)


MESH = pl.DeviceIdType.MESH
GATE, UP, DOWN = 0, 1, 2


def exchange_kernel(
    n_rep, n_fs, factor,
    tokens_ref, cotangent_ref, gate_ref, up_ref, down_ref,
    input_ref, gate_out, up_out, down_out, column_power, row_power,
    rows_all, gate_all, up_all, down_all,
    grad_gate, grad_up, hidden_all,
    normed_part, partner_part, rep_part,
    gate_send, up_send, down_send, gate_recv, up_recv, down_recv,
    column_parts, row_parts,
    rows_up, rows_down, rows_recv, pair_send, pair_recv,
    weight_ssem, weight_rsem,
    partner_ssem, partner_rsem, rep_ssem, rep_rsem,
    scatter_ssem, scatter_rsem,
    gather_up, gather_down, gather_rsem,
    column_ssem, column_rsem, row_ssem, row_rsem,
):
    z, f, t = lax.axis_index("rep"), lax.axis_index("fs"), lax.axis_index("tp")
    other = 1 - t
    local, width = tokens_ref.shape
    block = gate_ref.shape[0]
    hidden_units = gate_ref.shape[1]
    chunk = 2 * local

    def remote(source, target, send_sem, recv_sem, where):
        return pltpu.make_async_remote_copy(
            src_ref=source, dst_ref=target, send_sem=send_sem, recv_sem=recv_sem,
            device_id={"rep": where[0], "fs": where[1], "tp": where[2]},
            device_id_type=MESH,
        )

    def shifted(value, by, count):
        return lax.rem(value + by, count)

    barrier = pltpu.get_barrier_semaphore()

    def greet(where):
        pl.semaphore_signal(
            barrier, inc=1, device_id={"rep": where[0], "fs": where[1], "tp": where[2]},
            device_id_type=MESH,
        )

    for dz in range(n_rep):
        for df in range(n_fs):
            if dz or df:
                greet((shifted(z, dz, n_rep), shifted(f, df, n_fs), t))
        greet((shifted(z, dz, n_rep), f, other))

    def normalise():
        xfloat = tokens_ref[...].astype(jnp.float32)
        mean = jnp.sum(xfloat * xfloat, axis=1, keepdims=True) * (1.0 / width)
        recip_norm = lax.rsqrt(mean + EPSILON)
        return xfloat * recip_norm, recip_norm

    rows_all[z, t, 0] = normalise()[0].astype(jnp.bfloat16)
    rows_all[z, t, 1] = cotangent_ref[...]
    gate_all[f] = gate_ref[...]
    up_all[f] = up_ref[...]
    down_all[f] = down_ref[...]
    pl.semaphore_wait(barrier, n_rep * n_fs - 1 + n_rep)

    weights = ((gate_ref, gate_all), (up_ref, up_all), (down_ref, down_all))

    def weight_copy(which, d):
        source, target = weights[which]
        return remote(
            source, target.at[f], weight_ssem.at[which, d], weight_rsem.at[which, d],
            (z, shifted(f, d, n_fs), t),
        )

    def weight_arrival(which, d):
        source, target = weights[which]
        return remote(
            source, target.at[shifted(f, n_fs - d, n_fs)],
            weight_ssem.at[which, d], weight_rsem.at[which, d], (z, shifted(f, d, n_fs), t),
        )

    def row_copy(j, sems, to):
        return remote(
            rows_all.at[j, t], rows_all.at[j, t], sems.at[j], rows_recv.at[j], (to, f, t)
        )

    def pair_copy(j, half):
        return remote(
            rows_all.at[j, half], rows_all.at[j, half], pair_send.at[j], pair_recv.at[j],
            (z, f, other),
        )

    @pl.when(z < n_rep - 1)
    def _():
        row_copy(z, rows_up, z + 1).start()

    @pl.when(z > 0)
    def _():
        row_copy(z, rows_down, z - 1).start()

    for which in (GATE, UP, DOWN):
        for d in range(1, n_fs):
            weight_copy(which, d).start()
    pair_copy(z, t).start()

    for s in range(1, n_rep):
        @pl.when(z - s >= 0)
        def _():
            row_copy(z - s, rows_up, z).wait_recv()
            pair_copy(z - s, t).start()

            @pl.when(z < n_rep - 1)
            def _():
                row_copy(z - s, rows_up, z + 1).start()

        @pl.when(z + s < n_rep)
        def _():
            row_copy(z + s, rows_down, z).wait_recv()
            pair_copy(z + s, t).start()

            @pl.when(z > 0)
            def _():
                row_copy(z + s, rows_down, z - 1).start()

    for j in range(n_rep):
        pair_copy(j, other).wait_recv()
    for which in (GATE, UP, DOWN):
        for d in range(1, n_fs):
            weight_arrival(which, d).wait_recv()

    def forward(j, carry):
        normed = rows_all[j, :, 0].reshape(chunk, width)
        cotangent = rows_all[j, :, 1].reshape(chunk, width)
        gate_pre = jnp.dot(
            normed, gate_all[...].reshape(width, hidden_units), preferred_element_type=jnp.float32
        )
        up_pre = jnp.dot(
            normed, up_all[...].reshape(width, hidden_units), preferred_element_type=jnp.float32
        )
        grad_hidden = jnp.zeros((chunk, hidden_units), jnp.float32)
        for k in range(n_fs):
            grad_hidden += contract_cols(cotangent[:, k * block : (k + 1) * block], down_all[k])
        grad_hidden = 0.5 * grad_hidden
        sigmoid_gate = jax.nn.sigmoid(gate_pre)
        activated = gate_pre * sigmoid_gate
        at = pl.ds(pl.multiple_of(j * chunk, chunk), chunk)
        hidden_all[at, :] = (activated * up_pre).astype(jnp.bfloat16)
        grad_up_pre = (grad_hidden * activated).astype(jnp.bfloat16)
        grad_gate_pre = (
            grad_hidden * up_pre * sigmoid_gate * (1.0 + gate_pre * (1.0 - sigmoid_gate))
        ).astype(jnp.bfloat16)
        grad_up[at, :] = grad_up_pre
        grad_gate[at, :] = grad_gate_pre
        for k in range(n_fs):
            part = contract_cols(grad_gate_pre, gate_all[k]) + contract_cols(
                grad_up_pre, up_all[k]
            )
            normed_part[j, :, :, k * block : (k + 1) * block] = part.reshape(2, local, block)
        return carry

    lax.fori_loop(0, n_rep, forward, 0)

    def partner_copy(j):
        return remote(
            normed_part.at[j, other], partner_part.at[j], partner_ssem.at[j], partner_rsem.at[j],
            (z, f, other),
        )

    for j in range(n_rep):
        partner_copy(j).start()

    def columns_of(half, k):
        at = pl.ds(pl.multiple_of(k * block, block), block)
        return rows_all[:, :, half, :, at].reshape(n_rep * chunk, block)

    def term(which, k):
        if which == GATE:
            return contract_rows(columns_of(0, k), grad_gate[...])
        if which == UP:
            return contract_rows(columns_of(0, k), grad_up[...])
        return contract_rows(hidden_all[...], columns_of(1, k))

    sums = ((gate_send, gate_recv), (up_send, up_recv), (down_send, down_recv))

    def scatter_copy(which, d):
        source, target = sums[which]
        return remote(
            source.at[d], target.at[d], scatter_ssem.at[which, d], scatter_rsem.at[which, d],
            (z, shifted(f, d, n_fs), t),
        )

    def send_terms(which):
        for d in range(1, n_fs):
            sums[which][0][d] = term(which, shifted(f, d, n_fs))
            scatter_copy(which, d).start()

    def rep_copy(d):
        return remote(
            normed_part.at[shifted(z, d, n_rep), t], rep_part.at[d],
            rep_ssem.at[d], rep_rsem.at[d], (shifted(z, d, n_rep), f, t),
        )

    send_terms(GATE)
    for j in range(n_rep):
        partner_copy(j).wait_recv()
        normed_part[j, t] = normed_part[j, t] + partner_part[j]
    for d in range(1, n_rep):
        rep_copy(d).start()
    send_terms(UP)
    send_terms(DOWN)
    for which in (GATE, UP, DOWN):
        sums[which][0][0] = term(which, f)

    outs = (gate_out, up_out, down_out)

    def gather_copy(which, j, sems, to):
        return remote(
            outs[which].at[j], outs[which].at[j], sems.at[which, j], gather_rsem.at[which, j],
            (to, f, t),
        )

    def row_squares(value):
        return lax.dot_general(
            jnp.ones((8, value.shape[1]), jnp.float32), value * value,
            (((1,), (1,)), ((), ())), preferred_element_type=jnp.float32,
            precision=lax.Precision.HIGHEST,
        )

    def own_sum(which):
        source, target = sums[which]
        total = source[0]
        for d in range(1, n_fs):
            scatter_copy(which, d).wait_recv()
            total = total + target[d]
        total = total * (factor if which != DOWN else 0.5 * factor)
        outs[which][z] = total

        @pl.when(z < n_rep - 1)
        def _():
            gather_copy(which, z, gather_up, z + 1).start()

        @pl.when(z > 0)
        def _():
            gather_copy(which, z, gather_down, z - 1).start()

        if which == DOWN:
            row_parts[z, f] = row_squares(total)
        else:
            column_parts[z, t, which] = row_squares(total)

    def relay(which, s):
        @pl.when(z - s >= 0)
        def _():
            gather_copy(which, z - s, gather_up, z).wait_recv()

            @pl.when(z < n_rep - 1)
            def _():
                gather_copy(which, z - s, gather_up, z + 1).start()

        @pl.when(z + s < n_rep)
        def _():
            gather_copy(which, z + s, gather_down, z).wait_recv()

            @pl.when(z > 0)
            def _():
                gather_copy(which, z + s, gather_down, z - 1).start()

    def column_copy(dz, dt):
        return remote(
            column_parts.at[z, t], column_parts.at[z, t],
            column_ssem.at[dz, dt], column_rsem.at[dz, dt],
            (shifted(z, dz, n_rep), f, shifted(t, dt, 2)),
        )

    def column_arrival(dz, dt):
        at_z, at_t = shifted(z, n_rep - dz, n_rep), shifted(t, dt, 2)
        return remote(
            column_parts.at[z, t], column_parts.at[at_z, at_t],
            column_ssem.at[dz, dt], column_rsem.at[dz, dt],
            (shifted(z, dz, n_rep), f, shifted(t, dt, 2)),
        )

    def row_power_copy(dz, df):
        return remote(
            row_parts.at[z, f], row_parts.at[z, f], row_ssem.at[dz, df], row_rsem.at[dz, df],
            (shifted(z, dz, n_rep), shifted(f, df, n_fs), t),
        )

    def row_power_arrival(dz, df):
        at_z, at_f = shifted(z, n_rep - dz, n_rep), shifted(f, n_fs - df, n_fs)
        return remote(
            row_parts.at[z, f], row_parts.at[at_z, at_f], row_ssem.at[dz, df],
            row_rsem.at[dz, df], (shifted(z, dz, n_rep), shifted(f, df, n_fs), t),
        )

    column_peers = [(dz, dt) for dz in range(n_rep) for dt in range(2) if dz or dt]
    row_peers = [(dz, df) for dz in range(n_rep) for df in range(n_fs) if dz or df]

    own_sum(GATE)
    relay(GATE, 1)
    own_sum(UP)
    for peer in column_peers:
        column_copy(*peer).start()
    for s in range(2, n_rep):
        relay(GATE, s)
    relay(UP, 1)
    own_sum(DOWN)
    for peer in row_peers:
        row_power_copy(*peer).start()
    for s in range(2, n_rep):
        relay(UP, s)
    for s in range(1, n_rep):
        relay(DOWN, s)

    grad_normed = normed_part[z, t]
    for d in range(1, n_rep):
        rep_copy(d).wait_recv()
        grad_normed = grad_normed + rep_part[d]
    normed_exact, recip_norm = normalise()
    inner = jnp.sum(grad_normed * normed_exact, axis=1, keepdims=True) * (1.0 / width)
    input_ref[...] = (recip_norm * (grad_normed - normed_exact * inner)).astype(jnp.bfloat16)

    for peer in column_peers:
        column_arrival(*peer).wait_recv()
    for peer in row_peers:
        row_power_arrival(*peer).wait_recv()
    column_power[...] = jnp.sum(column_parts[...].reshape((2 * n_rep,) + column_parts.shape[2:]), axis=0)
    row_power[...] = jnp.sum(row_parts[...], axis=1)

    for which in (GATE, UP, DOWN):
        for d in range(1, n_fs):
            weight_copy(which, d).wait_send()
            scatter_copy(which, d).wait_send()
    for j in range(n_rep):
        pair_copy(j, t).wait_send()
        partner_copy(j).wait_send()

        @pl.when((z < n_rep - 1) & (z >= j))
        def _():
            row_copy(j, rows_up, z).wait_send()
            for which in (GATE, UP, DOWN):
                gather_copy(which, j, gather_up, z).wait_send()

        @pl.when((z > 0) & (z <= j))
        def _():
            row_copy(j, rows_down, z).wait_send()
            for which in (GATE, UP, DOWN):
                gather_copy(which, j, gather_down, z).wait_send()
    for d in range(1, n_rep):
        rep_copy(d).wait_send()
    for peer in column_peers:
        column_copy(*peer).wait_send()
    for peer in row_peers:
        row_power_copy(*peer).wait_send()


def on_device_fused(n_rep, n_fs, tokens, cotangent, gate_weight, up_weight, down_weight):
    local, width = tokens.shape
    block, hidden_local = gate_weight.shape
    units = hidden_local // n_rep
    factor = 1.0 / math.sqrt(local * 2 * n_rep * n_fs)
    start = lax.axis_index("rep") * units
    gate_part = lax.dynamic_slice_in_dim(gate_weight, start, units, axis=1)
    up_part = lax.dynamic_slice_in_dim(up_weight, start, units, axis=1)
    down_part = lax.dynamic_slice_in_dim(down_weight, start, units, axis=0)
    count = n_rep * 2 * local
    f32, bf16 = jnp.float32, jnp.bfloat16
    shapes = (
        jax.ShapeDtypeStruct((local, width), bf16),
        jax.ShapeDtypeStruct((n_rep, block, units), f32),
        jax.ShapeDtypeStruct((n_rep, block, units), f32),
        jax.ShapeDtypeStruct((n_rep, units, block), f32),
        jax.ShapeDtypeStruct((2, 8, block), f32),
        jax.ShapeDtypeStruct((n_rep, 8, units), f32),
    )
    dma = pltpu.SemaphoreType.DMA
    vmem = pltpu.VMEM
    scratch = [
        vmem((n_rep, 2, 2, local, width), bf16),
        vmem((n_fs, block, units), bf16),
        vmem((n_fs, block, units), bf16),
        vmem((n_fs, units, block), bf16),
        vmem((count, units), bf16),
        vmem((count, units), bf16),
        vmem((count, units), bf16),
        vmem((n_rep, 2, local, width), f32),
        vmem((n_rep, local, width), f32),
        vmem((n_rep, local, width), f32),
        vmem((n_fs, block, units), f32),
        vmem((n_fs, block, units), f32),
        vmem((n_fs, units, block), f32),
        vmem((n_fs, block, units), f32),
        vmem((n_fs, block, units), f32),
        vmem((n_fs, units, block), f32),
        vmem((n_rep, 2, 2, 8, block), f32),
        vmem((n_rep, n_fs, 8, units), f32),
        dma((n_rep,)), dma((n_rep,)), dma((n_rep,)), dma((n_rep,)), dma((n_rep,)),
        dma((3, n_fs)), dma((3, n_fs)),
        dma((n_rep,)), dma((n_rep,)), dma((n_rep,)), dma((n_rep,)),
        dma((3, n_fs)), dma((3, n_fs)),
        dma((3, n_rep)), dma((3, n_rep)), dma((3, n_rep)),
        dma((n_rep, 2)), dma((n_rep, 2)), dma((n_rep, n_fs)), dma((n_rep, n_fs)),
    ]
    whole = pl.BlockSpec(memory_space=pltpu.VMEM)
    input_grad, gate_blocks, up_blocks, down_blocks, column_power, row_power = pl.pallas_call(
        functools.partial(exchange_kernel, n_rep, n_fs, factor),
        out_shape=shapes,
        in_specs=[whole] * 5,
        out_specs=(whole,) * 6,
        scratch_shapes=scratch,
        compiler_params=pltpu.CompilerParams(
            collective_id=0, has_side_effects=True, vmem_limit_bytes=56 * 1024 * 1024
        ),
    )(tokens, cotangent, gate_part, up_part, down_part)
    hidden_units = hidden_local * 2
    return (
        input_grad,
        gate_blocks.transpose(1, 0, 2).reshape(block, hidden_local),
        up_blocks.transpose(1, 0, 2).reshape(block, hidden_local),
        down_blocks.reshape(hidden_local, block),
        column_power[0, 0] / hidden_units,
        column_power[1, 0] / hidden_units,
        row_power[:, 0].reshape(hidden_local) / width,
    )


def solution(mesh):
    placed = (
        P(("rep", "fs", "tp"), None),
        P(("rep", "fs", "tp"), None),
        P("fs", "tp"),
        P("fs", "tp"),
        P("tp", "fs"),
    )
    n_rep, n_fs = mesh.shape["rep"], mesh.shape["fs"]
    step = on_device
    if mesh.shape["tp"] == 2 and FF // 2 % (16 * n_rep) == 0 and D % (128 * n_fs) == 0:
        step = functools.partial(on_device_fused, n_rep, n_fs)
    return jax.shard_map(
        step,
        mesh=mesh,
        in_specs=placed,
        out_specs=(
            P(("rep", "fs", "tp"), None),
            P("fs", "tp"),
            P("fs", "tp"),
            P("tp", "fs"),
            P("fs"),
            P("fs"),
            P("tp"),
        ),
        check_vma=False,
    )
```

```python
import functools
import math

import jax
import jax.numpy as jnp
from jax import lax
from jax.experimental import pallas as pl
from jax.experimental.pallas import tpu as pltpu
from jax.sharding import PartitionSpec as P

D = 1024
FF = 2816


EPSILON = 1e-06


def contract_rows(left, right):
    return lax.dot_general(
        left, right, (((0,), (0,)), ((), ())), preferred_element_type=jnp.float32
    )


def contract_cols(left, right):
    return lax.dot_general(
        left, right, (((1,), (1,)), ((), ())), preferred_element_type=jnp.float32
    )


def on_device(tokens, cotangent, gate_weight, up_weight, down_weight):
    tp_count = lax.axis_size("tp")
    fs_count = lax.axis_size("fs")
    rep_count = lax.axis_size("rep")
    width = tokens.shape[1]
    factor = 1.0 / math.sqrt(tokens.shape[0] * tp_count * fs_count * rep_count)
    xfloat = tokens.astype(jnp.float32)
    recip_norm = lax.rsqrt(jnp.mean(xfloat * xfloat, axis=1, keepdims=True) + EPSILON)
    normed_exact = xfloat * recip_norm
    normed = normed_exact.astype(jnp.bfloat16)
    group_normed, group_cotangent = (
        lax.all_gather(normed, "tp", axis=0, tiled=True),
        lax.all_gather(cotangent, "tp", axis=0, tiled=True),
    )
    gate_full, up_full, down_full = (
        lax.all_gather(gate_weight, "fs", axis=0, tiled=True),
        lax.all_gather(up_weight, "fs", axis=0, tiled=True),
        lax.all_gather(down_weight.T, "fs", axis=0, tiled=True),
    )
    gate_pre = jnp.dot(group_normed, gate_full, preferred_element_type=jnp.float32)
    up_pre = jnp.dot(group_normed, up_full, preferred_element_type=jnp.float32)
    sigmoid_gate = jax.nn.sigmoid(gate_pre)
    activated = gate_pre * sigmoid_gate
    hidden = (activated * up_pre).astype(jnp.bfloat16)
    grad_hidden = 0.5 * jnp.dot(group_cotangent, down_full, preferred_element_type=jnp.float32)
    grad_up_pre = (grad_hidden * activated).astype(jnp.bfloat16)
    grad_gate_pre = (
        grad_hidden * up_pre * sigmoid_gate * (1.0 + gate_pre * (1.0 - sigmoid_gate))
    ).astype(jnp.bfloat16)
    normed_part = contract_cols(grad_gate_pre, gate_full) + contract_cols(grad_up_pre, up_full)
    grad_normed = lax.psum_scatter(normed_part, "tp", scatter_dimension=0, tiled=True)
    inner = jnp.mean(grad_normed * normed_exact, axis=1, keepdims=True)
    input_grad = (recip_norm * (grad_normed - normed_exact * inner)).astype(jnp.bfloat16)
    hidden_local = gate_weight.shape[1]

    def rows_term():
        normed_cols = lax.slice_in_dim(
            group_normed, 0, width // fs_count * lax.axis_size("fs"), axis=1
        )
        cotangent_cols = lax.slice_in_dim(
            group_cotangent, 0, width // fs_count * lax.axis_size("fs"), axis=1
        )
        return factor * jnp.concatenate(
            [
                contract_rows(normed_cols, grad_gate_pre),
                contract_rows(normed_cols, grad_up_pre),
                0.5 * contract_rows(cotangent_cols, hidden),
            ],
            axis=1,
        )

    reduced = lax.psum_scatter(rows_term(), "fs", scatter_dimension=0, tiled=True)
    reduced = lax.psum(reduced, "rep")
    gate_grad = reduced[:, :hidden_local]
    up_grad = reduced[:, hidden_local : 2 * hidden_local]
    down_grad = reduced[:, 2 * hidden_local :].T
    gate_sums, up_sums = lax.psum(
        (jnp.sum(gate_grad * gate_grad, axis=1), jnp.sum(up_grad * up_grad, axis=1)), "tp"
    )
    down_sums = lax.psum(jnp.sum(down_grad * down_grad, axis=1), "fs")
    return (input_grad, gate_grad, up_grad, down_grad, gate_sums / FF, up_sums / FF, down_sums / D)


MESH = pl.DeviceIdType.MESH
GATE, UP, DOWN = 0, 1, 2


def exchange_kernel(
    n_rep, n_fs, factor,
    tokens_ref, cotangent_ref, gate_ref, up_ref, down_ref,
    input_ref, gate_low, gate_high, up_low, up_high, down_low, down_high, column_power, row_power,
    rows_all, gate_all, up_all, down_all,
    grad_gate, grad_up, hidden_all,
    normed_part, partner_part, rep_part,
    gate_send, up_send, down_send, gate_recv, up_recv, down_recv,
    column_parts, row_parts,
    rows_up, rows_down, rows_recv, pair_send, pair_recv,
    weight_ssem, weight_rsem,
    partner_ssem, partner_rsem, rep_ssem, rep_rsem,
    scatter_ssem, scatter_rsem,
    gather_up, gather_down, gather_rsem,
    column_ssem, column_rsem, row_ssem, row_rsem,
):
    z, f, t = lax.axis_index("rep"), lax.axis_index("fs"), lax.axis_index("tp")
    other = 1 - t
    local, width = tokens_ref.shape
    block = gate_ref.shape[0]
    hidden_units = gate_all.shape[2]
    chunk = 2 * local

    def remote(source, target, send_sem, recv_sem, where):
        return pltpu.make_async_remote_copy(
            src_ref=source, dst_ref=target, send_sem=send_sem, recv_sem=recv_sem,
            device_id={"rep": where[0], "fs": where[1], "tp": where[2]},
            device_id_type=MESH,
        )

    def shifted(value, by, count):
        return lax.rem(value + by, count)

    barrier = pltpu.get_barrier_semaphore()

    def greet(where):
        pl.semaphore_signal(
            barrier, inc=1, device_id={"rep": where[0], "fs": where[1], "tp": where[2]},
            device_id_type=MESH,
        )

    for dz in range(n_rep):
        for df in range(n_fs):
            if dz or df:
                greet((shifted(z, dz, n_rep), shifted(f, df, n_fs), t))
        greet((shifted(z, dz, n_rep), f, other))

    def normalise():
        xfloat = tokens_ref[...].astype(jnp.float32)
        mean = jnp.sum(xfloat * xfloat, axis=1, keepdims=True) * (1.0 / width)
        recip_norm = lax.rsqrt(mean + EPSILON)
        return xfloat * recip_norm, recip_norm

    rows_all[z, t, 0] = normalise()[0].astype(jnp.bfloat16)
    rows_all[z, t, 1] = cotangent_ref[...]
    for j in range(n_rep):
        @pl.when(z == j)
        def _():
            gate_all[f] = gate_ref[:, j * hidden_units : (j + 1) * hidden_units]
            up_all[f] = up_ref[:, j * hidden_units : (j + 1) * hidden_units]

    units_at = pl.ds(pl.multiple_of(z * hidden_units, 16), hidden_units)
    down_all[f] = down_ref[units_at, :]
    pl.semaphore_wait(barrier, n_rep * n_fs - 1 + n_rep)

    weights = ((gate_all.at[f], gate_all), (up_all.at[f], up_all), (down_ref.at[units_at], down_all))

    def weight_copy(which, d):
        source, target = weights[which]
        return remote(
            source, target.at[f], weight_ssem.at[which, d], weight_rsem.at[which, d],
            (z, shifted(f, d, n_fs), t),
        )

    def weight_arrival(which, d):
        source, target = weights[which]
        return remote(
            source, target.at[shifted(f, n_fs - d, n_fs)],
            weight_ssem.at[which, d], weight_rsem.at[which, d], (z, shifted(f, d, n_fs), t),
        )

    def row_copy(j, sems, to):
        return remote(
            rows_all.at[j, t], rows_all.at[j, t], sems.at[j], rows_recv.at[j], (to, f, t)
        )

    def pair_copy(j, half):
        return remote(
            rows_all.at[j, half], rows_all.at[j, half], pair_send.at[j], pair_recv.at[j],
            (z, f, other),
        )

    @pl.when(z < n_rep - 1)
    def _():
        row_copy(z, rows_up, z + 1).start()

    @pl.when(z > 0)
    def _():
        row_copy(z, rows_down, z - 1).start()

    for which in (GATE, UP, DOWN):
        for d in range(1, n_fs):
            weight_copy(which, d).start()
    pair_copy(z, t).start()

    for s in range(1, n_rep):
        @pl.when(z - s >= 0)
        def _():
            row_copy(z - s, rows_up, z).wait_recv()
            pair_copy(z - s, t).start()

            @pl.when(z < n_rep - 1)
            def _():
                row_copy(z - s, rows_up, z + 1).start()

        @pl.when(z + s < n_rep)
        def _():
            row_copy(z + s, rows_down, z).wait_recv()
            pair_copy(z + s, t).start()

            @pl.when(z > 0)
            def _():
                row_copy(z + s, rows_down, z - 1).start()

    for j in range(n_rep):
        pair_copy(j, other).wait_recv()
    for which in (GATE, UP, DOWN):
        for d in range(1, n_fs):
            weight_arrival(which, d).wait_recv()

    def forward(j, carry):
        normed = rows_all[j, :, 0].reshape(chunk, width)
        cotangent = rows_all[j, :, 1].reshape(chunk, width)
        gate_pre = jnp.dot(
            normed, gate_all[...].reshape(width, hidden_units), preferred_element_type=jnp.float32
        )
        up_pre = jnp.dot(
            normed, up_all[...].reshape(width, hidden_units), preferred_element_type=jnp.float32
        )
        grad_hidden = jnp.zeros((chunk, hidden_units), jnp.float32)
        for k in range(n_fs):
            grad_hidden += contract_cols(cotangent[:, k * block : (k + 1) * block], down_all[k])
        grad_hidden = 0.5 * grad_hidden
        sigmoid_gate = jax.nn.sigmoid(gate_pre)
        activated = gate_pre * sigmoid_gate
        at = pl.ds(pl.multiple_of(j * chunk, chunk), chunk)
        hidden_all[at, :] = (activated * up_pre).astype(jnp.bfloat16)
        grad_up_pre = (grad_hidden * activated).astype(jnp.bfloat16)
        grad_gate_pre = (
            grad_hidden * up_pre * sigmoid_gate * (1.0 + gate_pre * (1.0 - sigmoid_gate))
        ).astype(jnp.bfloat16)
        grad_up[at, :] = grad_up_pre
        grad_gate[at, :] = grad_gate_pre
        for k in range(n_fs):
            part = contract_cols(grad_gate_pre, gate_all[k]) + contract_cols(
                grad_up_pre, up_all[k]
            )
            normed_part[j, :, :, k * block : (k + 1) * block] = part.reshape(2, local, block)
        return carry

    lax.fori_loop(0, n_rep, forward, 0)

    def partner_copy(j):
        return remote(
            normed_part.at[j, other], partner_part.at[j], partner_ssem.at[j], partner_rsem.at[j],
            (z, f, other),
        )

    for j in range(n_rep):
        partner_copy(j).start()

    def columns_of(half, k):
        at = pl.ds(pl.multiple_of(k * block, block), block)
        return rows_all[:, :, half, :, at].reshape(n_rep * chunk, block)

    def term(which, k):
        if which == GATE:
            return contract_rows(columns_of(0, k), grad_gate[...])
        if which == UP:
            return contract_rows(columns_of(0, k), grad_up[...])
        return contract_rows(hidden_all[...], columns_of(1, k))

    sums = ((gate_send, gate_recv), (up_send, up_recv), (down_send, down_recv))

    def scatter_copy(which, d):
        source, target = sums[which]
        return remote(
            source.at[d], target.at[d], scatter_ssem.at[which, d], scatter_rsem.at[which, d],
            (z, shifted(f, d, n_fs), t),
        )

    def send_terms(which):
        for d in range(1, n_fs):
            sums[which][0][d] = term(which, shifted(f, d, n_fs))
            scatter_copy(which, d).start()

    def rep_copy(d):
        return remote(
            normed_part.at[shifted(z, d, n_rep), t], rep_part.at[d],
            rep_ssem.at[d], rep_rsem.at[d], (shifted(z, d, n_rep), f, t),
        )

    send_terms(GATE)
    for j in range(n_rep):
        partner_copy(j).wait_recv()
        normed_part[j, t] = normed_part[j, t] + partner_part[j]
    for d in range(1, n_rep):
        rep_copy(d).start()
    send_terms(UP)
    send_terms(DOWN)
    for which in (GATE, UP, DOWN):
        sums[which][0][0] = term(which, f)

    outs = ((gate_low, gate_high), (up_low, up_high), (down_low, down_high))

    class gather_copy:
        def __init__(self, which, j, sems, to):
            self.pieces = [
                remote(
                    out.at[j], out.at[j], sems.at[which, part, j],
                    gather_rsem.at[which, part, j], (to, f, t),
                )
                for part, out in enumerate(outs[which])
            ]

        def start(self):
            for piece in self.pieces:
                piece.start()

        def wait_recv(self):
            for piece in self.pieces:
                piece.wait_recv()

        def wait_send(self):
            for piece in self.pieces:
                piece.wait_send()

    def row_squares(value):
        return lax.dot_general(
            jnp.ones((8, value.shape[1]), jnp.float32), value * value,
            (((1,), (1,)), ((), ())), preferred_element_type=jnp.float32,
            precision=lax.Precision.HIGHEST,
        )

    def own_sum(which):
        source, target = sums[which]
        total = source[0]
        for d in range(1, n_fs):
            scatter_copy(which, d).wait_recv()
            total = total + target[d]
        total = total * (factor if which != DOWN else 0.5 * factor)
        cut = outs[which][0].shape[1]
        outs[which][0][z] = total[:cut].astype(jnp.bfloat16)
        outs[which][1][z] = total[cut:]

        @pl.when(z < n_rep - 1)
        def _():
            gather_copy(which, z, gather_up, z + 1).start()

        @pl.when(z > 0)
        def _():
            gather_copy(which, z, gather_down, z - 1).start()

        if which == DOWN:
            row_parts[z, f] = row_squares(total)
        else:
            column_parts[z, t, which] = row_squares(total)

    def relay(which, s):
        @pl.when(z - s >= 0)
        def _():
            gather_copy(which, z - s, gather_up, z).wait_recv()

            @pl.when(z < n_rep - 1)
            def _():
                gather_copy(which, z - s, gather_up, z + 1).start()

        @pl.when(z + s < n_rep)
        def _():
            gather_copy(which, z + s, gather_down, z).wait_recv()

            @pl.when(z > 0)
            def _():
                gather_copy(which, z + s, gather_down, z - 1).start()

    def column_copy(dz, dt):
        return remote(
            column_parts.at[z, t], column_parts.at[z, t],
            column_ssem.at[dz, dt], column_rsem.at[dz, dt],
            (shifted(z, dz, n_rep), f, shifted(t, dt, 2)),
        )

    def column_arrival(dz, dt):
        at_z, at_t = shifted(z, n_rep - dz, n_rep), shifted(t, dt, 2)
        return remote(
            column_parts.at[z, t], column_parts.at[at_z, at_t],
            column_ssem.at[dz, dt], column_rsem.at[dz, dt],
            (shifted(z, dz, n_rep), f, shifted(t, dt, 2)),
        )

    def row_power_copy(dz, df):
        return remote(
            row_parts.at[z, f], row_parts.at[z, f], row_ssem.at[dz, df], row_rsem.at[dz, df],
            (shifted(z, dz, n_rep), shifted(f, df, n_fs), t),
        )

    def row_power_arrival(dz, df):
        at_z, at_f = shifted(z, n_rep - dz, n_rep), shifted(f, n_fs - df, n_fs)
        return remote(
            row_parts.at[z, f], row_parts.at[at_z, at_f], row_ssem.at[dz, df],
            row_rsem.at[dz, df], (shifted(z, dz, n_rep), shifted(f, df, n_fs), t),
        )

    column_peers = [(dz, dt) for dz in range(n_rep) for dt in range(2) if dz or dt]
    row_peers = [(dz, df) for dz in range(n_rep) for df in range(n_fs) if dz or df]

    own_sum(GATE)
    relay(GATE, 1)
    own_sum(UP)
    for peer in column_peers:
        column_copy(*peer).start()
    for s in range(2, n_rep):
        relay(GATE, s)
    relay(UP, 1)
    own_sum(DOWN)
    for peer in row_peers:
        row_power_copy(*peer).start()
    for s in range(2, n_rep):
        relay(UP, s)
    for s in range(1, n_rep):
        relay(DOWN, s)

    grad_normed = normed_part[z, t]
    for d in range(1, n_rep):
        rep_copy(d).wait_recv()
        grad_normed = grad_normed + rep_part[d]
    normed_exact, recip_norm = normalise()
    inner = jnp.sum(grad_normed * normed_exact, axis=1, keepdims=True) * (1.0 / width)
    input_ref[...] = (recip_norm * (grad_normed - normed_exact * inner)).astype(jnp.bfloat16)

    for peer in column_peers:
        column_arrival(*peer).wait_recv()
    for peer in row_peers:
        row_power_arrival(*peer).wait_recv()
    column_power[...] = jnp.sum(column_parts[...].reshape((2 * n_rep,) + column_parts.shape[2:]), axis=0)
    row_power[...] = jnp.sum(row_parts[...], axis=1)

    for which in (GATE, UP, DOWN):
        for d in range(1, n_fs):
            weight_copy(which, d).wait_send()
            scatter_copy(which, d).wait_send()
    for j in range(n_rep):
        pair_copy(j, t).wait_send()
        partner_copy(j).wait_send()

        @pl.when((z < n_rep - 1) & (z >= j))
        def _():
            row_copy(j, rows_up, z).wait_send()
            for which in (GATE, UP, DOWN):
                gather_copy(which, j, gather_up, z).wait_send()

        @pl.when((z > 0) & (z <= j))
        def _():
            row_copy(j, rows_down, z).wait_send()
            for which in (GATE, UP, DOWN):
                gather_copy(which, j, gather_down, z).wait_send()
    for d in range(1, n_rep):
        rep_copy(d).wait_send()
    for peer in column_peers:
        column_copy(*peer).wait_send()
    for peer in row_peers:
        row_power_copy(*peer).wait_send()


def assemble_kernel(
    n_rep, width,
    gate_low, gate_high, up_low, up_high, down_low, down_high, column_power, row_power,
    gate_out, up_out, down_out, gate_power, up_power, down_power,
):
    cut, units = gate_low.shape[1:]
    down_cut = down_low.shape[1]
    for j in range(n_rep):
        at = slice(j * units, (j + 1) * units)
        for low, high, out in ((gate_low, gate_high, gate_out), (up_low, up_high, up_out)):
            out[:cut, at] = low[j].astype(jnp.float32)
            out[cut:, at] = high[j]
        down_out[j * units : j * units + down_cut, :] = down_low[j].astype(jnp.float32)
        down_out[j * units + down_cut : (j + 1) * units, :] = down_high[j]
        down_power[:, at] = row_power[j, 0:1] * (1.0 / width)
    gate_power[...] = column_power[0, 0:1] * (1.0 / (2 * n_rep * units))
    up_power[...] = column_power[1, 0:1] * (1.0 / (2 * n_rep * units))


def on_device_fused(n_rep, n_fs, tokens, cotangent, gate_weight, up_weight, down_weight):
    local, width = tokens.shape
    block, hidden_local = gate_weight.shape
    units = hidden_local // n_rep
    factor = 1.0 / math.sqrt(local * 2 * n_rep * n_fs)
    count = n_rep * 2 * local
    cut, down_cut = block * 3 // 4 // 16 * 16, units * 3 // 4 // 16 * 16
    f32, bf16 = jnp.float32, jnp.bfloat16
    shapes = (
        jax.ShapeDtypeStruct((local, width), bf16),
        jax.ShapeDtypeStruct((n_rep, cut, units), bf16),
        jax.ShapeDtypeStruct((n_rep, block - cut, units), f32),
        jax.ShapeDtypeStruct((n_rep, cut, units), bf16),
        jax.ShapeDtypeStruct((n_rep, block - cut, units), f32),
        jax.ShapeDtypeStruct((n_rep, down_cut, block), bf16),
        jax.ShapeDtypeStruct((n_rep, units - down_cut, block), f32),
        jax.ShapeDtypeStruct((2, 8, block), f32),
        jax.ShapeDtypeStruct((n_rep, 8, units), f32),
    )
    dma = pltpu.SemaphoreType.DMA
    vmem = pltpu.VMEM
    scratch = [
        vmem((n_rep, 2, 2, local, width), bf16),
        vmem((n_fs, block, units), bf16),
        vmem((n_fs, block, units), bf16),
        vmem((n_fs, units, block), bf16),
        vmem((count, units), bf16),
        vmem((count, units), bf16),
        vmem((count, units), bf16),
        vmem((n_rep, 2, local, width), f32),
        vmem((n_rep, local, width), f32),
        vmem((n_rep, local, width), f32),
        vmem((n_fs, block, units), f32),
        vmem((n_fs, block, units), f32),
        vmem((n_fs, units, block), f32),
        vmem((n_fs, block, units), f32),
        vmem((n_fs, block, units), f32),
        vmem((n_fs, units, block), f32),
        vmem((n_rep, 2, 2, 8, block), f32),
        vmem((n_rep, n_fs, 8, units), f32),
        dma((n_rep,)), dma((n_rep,)), dma((n_rep,)), dma((n_rep,)), dma((n_rep,)),
        dma((3, n_fs)), dma((3, n_fs)),
        dma((n_rep,)), dma((n_rep,)), dma((n_rep,)), dma((n_rep,)),
        dma((3, n_fs)), dma((3, n_fs)),
        dma((3, 2, n_rep)), dma((3, 2, n_rep)), dma((3, 2, n_rep)),
        dma((n_rep, 2)), dma((n_rep, 2)), dma((n_rep, n_fs)), dma((n_rep, n_fs)),
    ]
    whole = pl.BlockSpec(memory_space=pltpu.VMEM)
    input_grad, *blocks = pl.pallas_call(
        functools.partial(exchange_kernel, n_rep, n_fs, factor),
        out_shape=shapes,
        in_specs=[whole] * 5,
        out_specs=(whole,) * 9,
        scratch_shapes=scratch,
        compiler_params=pltpu.CompilerParams(
            collective_id=0, has_side_effects=True, vmem_limit_bytes=56 * 1024 * 1024
        ),
    )(tokens, cotangent, gate_weight, up_weight, down_weight)
    gate_grad, up_grad, down_grad, gate_power, up_power, down_power = pl.pallas_call(
        functools.partial(assemble_kernel, n_rep, width),
        out_shape=(
            jax.ShapeDtypeStruct((block, hidden_local), f32),
            jax.ShapeDtypeStruct((block, hidden_local), f32),
            jax.ShapeDtypeStruct((hidden_local, block), f32),
            jax.ShapeDtypeStruct((1, block), f32),
            jax.ShapeDtypeStruct((1, block), f32),
            jax.ShapeDtypeStruct((1, hidden_local), f32),
        ),
        in_specs=[whole] * 8,
        out_specs=(whole,) * 6,
        compiler_params=pltpu.CompilerParams(vmem_limit_bytes=32 * 1024 * 1024),
    )(*blocks)
    return (
        input_grad, gate_grad, up_grad, down_grad,
        gate_power.reshape(block), up_power.reshape(block), down_power.reshape(hidden_local),
    )


def solution(mesh):
    placed = (
        P(("rep", "fs", "tp"), None),
        P(("rep", "fs", "tp"), None),
        P("fs", "tp"),
        P("fs", "tp"),
        P("tp", "fs"),
    )
    n_rep, n_fs = mesh.shape["rep"], mesh.shape["fs"]
    step = on_device
    if mesh.shape["tp"] == 2 and FF // 2 % (16 * n_rep) == 0 and D % (128 * n_fs) == 0:
        step = functools.partial(on_device_fused, n_rep, n_fs)
    return jax.shard_map(
        step,
        mesh=mesh,
        in_specs=placed,
        out_specs=(
            P(("rep", "fs", "tp"), None),
            P("fs", "tp"),
            P("fs", "tp"),
            P("tp", "fs"),
            P("fs"),
            P("fs"),
            P("tp"),
        ),
        check_vma=False,
    )
```

```python
import functools
import math

import jax
import jax.numpy as jnp
from jax import lax
from jax.experimental import pallas as pl
from jax.experimental.pallas import tpu as pltpu
from jax.sharding import PartitionSpec as P

D = 1024
FF = 2816


EPSILON = 1e-06


def contract_rows(left, right):
    return lax.dot_general(
        left, right, (((0,), (0,)), ((), ())), preferred_element_type=jnp.float32
    )


def contract_cols(left, right):
    return lax.dot_general(
        left, right, (((1,), (1,)), ((), ())), preferred_element_type=jnp.float32
    )


def on_device(tokens, cotangent, gate_weight, up_weight, down_weight):
    tp_count = lax.axis_size("tp")
    fs_count = lax.axis_size("fs")
    rep_count = lax.axis_size("rep")
    width = tokens.shape[1]
    factor = 1.0 / math.sqrt(tokens.shape[0] * tp_count * fs_count * rep_count)
    xfloat = tokens.astype(jnp.float32)
    recip_norm = lax.rsqrt(jnp.mean(xfloat * xfloat, axis=1, keepdims=True) + EPSILON)
    normed_exact = xfloat * recip_norm
    normed = normed_exact.astype(jnp.bfloat16)
    group_normed, group_cotangent = (
        lax.all_gather(normed, "tp", axis=0, tiled=True),
        lax.all_gather(cotangent, "tp", axis=0, tiled=True),
    )
    gate_full, up_full, down_full = (
        lax.all_gather(gate_weight, "fs", axis=0, tiled=True),
        lax.all_gather(up_weight, "fs", axis=0, tiled=True),
        lax.all_gather(down_weight.T, "fs", axis=0, tiled=True),
    )
    gate_pre = jnp.dot(group_normed, gate_full, preferred_element_type=jnp.float32)
    up_pre = jnp.dot(group_normed, up_full, preferred_element_type=jnp.float32)
    sigmoid_gate = jax.nn.sigmoid(gate_pre)
    activated = gate_pre * sigmoid_gate
    hidden = (activated * up_pre).astype(jnp.bfloat16)
    grad_hidden = 0.5 * jnp.dot(group_cotangent, down_full, preferred_element_type=jnp.float32)
    grad_up_pre = (grad_hidden * activated).astype(jnp.bfloat16)
    grad_gate_pre = (
        grad_hidden * up_pre * sigmoid_gate * (1.0 + gate_pre * (1.0 - sigmoid_gate))
    ).astype(jnp.bfloat16)
    normed_part = contract_cols(grad_gate_pre, gate_full) + contract_cols(grad_up_pre, up_full)
    grad_normed = lax.psum_scatter(normed_part, "tp", scatter_dimension=0, tiled=True)
    inner = jnp.mean(grad_normed * normed_exact, axis=1, keepdims=True)
    input_grad = (recip_norm * (grad_normed - normed_exact * inner)).astype(jnp.bfloat16)
    hidden_local = gate_weight.shape[1]

    def rows_term():
        normed_cols = lax.slice_in_dim(
            group_normed, 0, width // fs_count * lax.axis_size("fs"), axis=1
        )
        cotangent_cols = lax.slice_in_dim(
            group_cotangent, 0, width // fs_count * lax.axis_size("fs"), axis=1
        )
        return factor * jnp.concatenate(
            [
                contract_rows(normed_cols, grad_gate_pre),
                contract_rows(normed_cols, grad_up_pre),
                0.5 * contract_rows(cotangent_cols, hidden),
            ],
            axis=1,
        )

    reduced = lax.psum_scatter(rows_term(), "fs", scatter_dimension=0, tiled=True)
    reduced = lax.psum(reduced, "rep")
    gate_grad = reduced[:, :hidden_local]
    up_grad = reduced[:, hidden_local : 2 * hidden_local]
    down_grad = reduced[:, 2 * hidden_local :].T
    gate_sums, up_sums = lax.psum(
        (jnp.sum(gate_grad * gate_grad, axis=1), jnp.sum(up_grad * up_grad, axis=1)), "tp"
    )
    down_sums = lax.psum(jnp.sum(down_grad * down_grad, axis=1), "fs")
    return (input_grad, gate_grad, up_grad, down_grad, gate_sums / FF, up_sums / FF, down_sums / D)


MESH = pl.DeviceIdType.MESH
GATE, UP, DOWN = 0, 1, 2


def exchange_kernel(
    n_rep, n_fs, factor,
    tokens_ref, cotangent_ref, gate_ref, up_ref, down_ref,
    input_ref, gate_low, gate_high, up_low, up_high, down_low, down_high, column_power, row_power,
    rows_all, gate_all, up_all, down_all,
    grad_gate, grad_up, hidden_all,
    normed_part, partner_part, rep_part,
    gate_send, up_send, down_send, gate_recv, up_recv, down_recv,
    column_parts, row_parts,
    rows_up, rows_down, rows_recv, pair_send, pair_recv,
    weight_ssem, weight_rsem,
    partner_ssem, partner_rsem, rep_ssem, rep_rsem,
    scatter_ssem, scatter_rsem,
    gather_up, gather_down, gather_rsem,
    column_ssem, column_rsem, row_ssem, row_rsem,
):
    z, f, t = lax.axis_index("rep"), lax.axis_index("fs"), lax.axis_index("tp")
    other = 1 - t
    side_x = f + 1 - 2 * lax.rem(f, 2)
    side_y = lax.rem(f + 2, n_fs)
    across = lax.rem(side_x + 2, n_fs)
    sides = (side_x, side_y)
    local, width = tokens_ref.shape
    block = gate_ref.shape[0]
    hidden_units = gate_all.shape[2]
    chunk = 2 * local

    def remote(source, target, send_sem, recv_sem, where):
        return pltpu.make_async_remote_copy(
            src_ref=source, dst_ref=target, send_sem=send_sem, recv_sem=recv_sem,
            device_id={"rep": where[0], "fs": where[1], "tp": where[2]},
            device_id_type=MESH,
        )

    def shifted(value, by, count):
        return lax.rem(value + by, count)

    barrier = pltpu.get_barrier_semaphore()

    def greet(where):
        pl.semaphore_signal(
            barrier, inc=1, device_id={"rep": where[0], "fs": where[1], "tp": where[2]},
            device_id_type=MESH,
        )

    for dz in range(n_rep):
        for df in range(n_fs):
            if dz or df:
                greet((shifted(z, dz, n_rep), shifted(f, df, n_fs), t))
        greet((shifted(z, dz, n_rep), f, other))

    def normalise():
        xfloat = tokens_ref[...].astype(jnp.float32)
        mean = jnp.sum(xfloat * xfloat, axis=1, keepdims=True) * (1.0 / width)
        recip_norm = lax.rsqrt(mean + EPSILON)
        return xfloat * recip_norm, recip_norm

    rows_all[z, t, 0] = normalise()[0].astype(jnp.bfloat16)
    rows_all[z, t, 1] = cotangent_ref[...]
    for j in range(n_rep):
        @pl.when(z == j)
        def _():
            gate_all[f] = gate_ref[:, j * hidden_units : (j + 1) * hidden_units]
            up_all[f] = up_ref[:, j * hidden_units : (j + 1) * hidden_units]

    units_at = pl.ds(pl.multiple_of(z * hidden_units, 16), hidden_units)
    down_all[f] = down_ref[units_at, :]
    pl.semaphore_wait(barrier, n_rep * n_fs - 1 + n_rep)

    weights = ((gate_all.at[f], gate_all), (up_all.at[f], up_all), (down_ref.at[units_at], down_all))

    def weight_copy(which, side):
        source, target = weights[which]
        return remote(
            source, target.at[f], weight_ssem.at[which, side], weight_rsem.at[which, side],
            (z, sides[side], t),
        )

    def weight_arrival(which, side):
        target = weights[which][1].at[sides[side]]
        return remote(
            target, target, weight_ssem.at[which, side], weight_rsem.at[which, side],
            (z, sides[side], t),
        )

    def half_of(which, part):
        rows = weights[which][1].shape[1] // 2
        return pl.ds(part * rows, rows)

    def weight_forward(which, side):
        origin = sides[1 - side]
        part = weights[which][1].at[origin, half_of(which, 1 - side)]
        return remote(
            part, part, weight_ssem.at[which, 2 + side], weight_rsem.at[which, 2 + side],
            (z, sides[side], t),
        )

    def weight_across(which, side):
        part = weights[which][1].at[across, half_of(which, 1 - side)]
        return remote(
            part, part, weight_ssem.at[which, 2 + side], weight_rsem.at[which, 2 + side],
            (z, sides[side], t),
        )

    def pass_weights(which):
        for side in (0, 1):
            weight_arrival(which, side).wait_recv()
            weight_forward(which, 1 - side).start()

    def row_copy(j, sems, to):
        return remote(
            rows_all.at[j, t], rows_all.at[j, t], sems.at[j], rows_recv.at[j], (to, f, t)
        )

    def pair_copy(j, half):
        return remote(
            rows_all.at[j, half], rows_all.at[j, half], pair_send.at[j], pair_recv.at[j],
            (z, f, other),
        )

    @pl.when(z < n_rep - 1)
    def _():
        row_copy(z, rows_up, z + 1).start()

    @pl.when(z > 0)
    def _():
        row_copy(z, rows_down, z - 1).start()

    for which in (GATE, UP, DOWN):
        for side in (0, 1):
            weight_copy(which, side).start()
    pair_copy(z, t).start()

    for s in range(1, max(n_rep, 4)):
        if s <= 3:
            pass_weights(s - 1)
        if s >= n_rep:
            continue

        @pl.when(z - s >= 0)
        def _():
            row_copy(z - s, rows_up, z).wait_recv()
            pair_copy(z - s, t).start()

            @pl.when(z < n_rep - 1)
            def _():
                row_copy(z - s, rows_up, z + 1).start()

        @pl.when(z + s < n_rep)
        def _():
            row_copy(z + s, rows_down, z).wait_recv()
            pair_copy(z + s, t).start()

            @pl.when(z > 0)
            def _():
                row_copy(z + s, rows_down, z - 1).start()

    for j in range(n_rep):
        pair_copy(j, other).wait_recv()
    for which in (GATE, UP, DOWN):
        for side in (0, 1):
            weight_across(which, side).wait_recv()

    def forward(j, carry):
        normed = rows_all[j, :, 0].reshape(chunk, width)
        cotangent = rows_all[j, :, 1].reshape(chunk, width)
        gate_pre = jnp.dot(
            normed, gate_all[...].reshape(width, hidden_units), preferred_element_type=jnp.float32
        )
        up_pre = jnp.dot(
            normed, up_all[...].reshape(width, hidden_units), preferred_element_type=jnp.float32
        )
        grad_hidden = jnp.zeros((chunk, hidden_units), jnp.float32)
        for k in range(n_fs):
            grad_hidden += contract_cols(cotangent[:, k * block : (k + 1) * block], down_all[k])
        grad_hidden = 0.5 * grad_hidden
        sigmoid_gate = jax.nn.sigmoid(gate_pre)
        activated = gate_pre * sigmoid_gate
        at = pl.ds(pl.multiple_of(j * chunk, chunk), chunk)
        hidden_all[at, :] = (activated * up_pre).astype(jnp.bfloat16)
        grad_up_pre = (grad_hidden * activated).astype(jnp.bfloat16)
        grad_gate_pre = (
            grad_hidden * up_pre * sigmoid_gate * (1.0 + gate_pre * (1.0 - sigmoid_gate))
        ).astype(jnp.bfloat16)
        grad_up[at, :] = grad_up_pre
        grad_gate[at, :] = grad_gate_pre
        return carry

    lax.fori_loop(0, n_rep, forward, 0)

    def backward(j, carry):
        at = pl.ds(pl.multiple_of(j * chunk, chunk), chunk)
        for k in range(n_fs):
            part = contract_cols(grad_gate[at, :], gate_all[k]) + contract_cols(
                grad_up[at, :], up_all[k]
            )
            normed_part[j, :, :, k * block : (k + 1) * block] = part.reshape(2, local, block)
        return carry

    def partner_copy(j):
        return remote(
            normed_part.at[j, other], partner_part.at[j], partner_ssem.at[j], partner_rsem.at[j],
            (z, f, other),
        )

    def columns_of(half, k):
        at = pl.ds(pl.multiple_of(k * block, block), block)
        return rows_all[:, :, half, :, at].reshape(n_rep * chunk, block)

    def term(which, k):
        if which == GATE:
            return contract_rows(columns_of(0, k), grad_gate[...])
        if which == UP:
            return contract_rows(columns_of(0, k), grad_up[...])
        return contract_rows(hidden_all[...], columns_of(1, k))

    sums = ((gate_send, gate_recv), (up_send, up_recv), (down_send, down_recv))

    def half(which, part):
        rows = sums[which][0].shape[1] // 2
        return pl.ds(part * rows, rows)

    def scatter_copy(which, side, kind):
        source, target = sums[which]
        at = half(which, side)
        slot = (1 + side) if kind == 0 else 3
        sem = 2 * side + kind
        return remote(
            source.at[slot, at], target.at[kind, at],
            scatter_ssem.at[which, sem], scatter_rsem.at[which, sem], (z, sides[side], t),
        )

    def pass_copy(which, side):
        source, target = sums[which]
        at = half(which, 1 - side)
        return remote(
            source.at[1 + side, at], target.at[2, at],
            scatter_ssem.at[which, 4 + side], scatter_rsem.at[which, 4 + side],
            (z, sides[side], t),
        )

    def send_terms(which):
        sums[which][0][3] = term(which, across)
        for side in (0, 1):
            scatter_copy(which, side, 1).start()
        for side in (0, 1):
            sums[which][0][1 + side] = term(which, sides[side])
            scatter_copy(which, side, 0).start()

    def pass_sums(which):
        source, target = sums[which]
        for side in (0, 1):
            scatter_copy(which, 1 - side, 1).wait_recv()
            at = half(which, 1 - side)
            source[1 + side, at] = source[1 + side, at] + target[1, at]
            pass_copy(which, side).start()

    def rep_copy(d):
        return remote(
            normed_part.at[shifted(z, d, n_rep), t], rep_part.at[d],
            rep_ssem.at[d], rep_rsem.at[d], (shifted(z, d, n_rep), f, t),
        )

    send_terms(GATE)
    lax.fori_loop(0, n_rep, backward, 0)
    for j in range(n_rep):
        partner_copy(j).start()
    send_terms(UP)
    for j in range(n_rep):
        partner_copy(j).wait_recv()
        normed_part[j, t] = normed_part[j, t] + partner_part[j]
    for d in range(1, n_rep):
        rep_copy(d).start()
    sums[GATE][0][0] = term(GATE, f)
    pass_sums(GATE)
    send_terms(DOWN)
    for which in (UP, DOWN):
        sums[which][0][0] = term(which, f)

    outs = ((gate_low, gate_high), (up_low, up_high), (down_low, down_high))

    class gather_copy:
        def __init__(self, which, j, sems, to):
            self.pieces = [
                remote(
                    out.at[j], out.at[j], sems.at[which, part, j],
                    gather_rsem.at[which, part, j], (to, f, t),
                )
                for part, out in enumerate(outs[which])
            ]

        def start(self):
            for piece in self.pieces:
                piece.start()

        def wait_recv(self):
            for piece in self.pieces:
                piece.wait_recv()

        def wait_send(self):
            for piece in self.pieces:
                piece.wait_send()

    def row_squares(value):
        return lax.dot_general(
            jnp.ones((8, value.shape[1]), jnp.float32), value * value,
            (((1,), (1,)), ((), ())), preferred_element_type=jnp.float32,
            precision=lax.Precision.HIGHEST,
        )

    def own_sum(which):
        source, target = sums[which]
        for side in (0, 1):
            scatter_copy(which, side, 0).wait_recv()
            pass_copy(which, side).wait_recv()
        total = source[0] + target[0] + target[2]
        total = total * (factor if which != DOWN else 0.5 * factor)
        cut = outs[which][0].shape[1]
        outs[which][0][z] = total[:cut].astype(jnp.bfloat16)
        outs[which][1][z] = total[cut:]

        @pl.when(z < n_rep - 1)
        def _():
            gather_copy(which, z, gather_up, z + 1).start()

        @pl.when(z > 0)
        def _():
            gather_copy(which, z, gather_down, z - 1).start()

        if which == DOWN:
            row_parts[z, f] = row_squares(total)
        else:
            column_parts[z, t, which] = row_squares(total)

    def relay(which, s):
        @pl.when(z - s >= 0)
        def _():
            gather_copy(which, z - s, gather_up, z).wait_recv()

            @pl.when(z < n_rep - 1)
            def _():
                gather_copy(which, z - s, gather_up, z + 1).start()

        @pl.when(z + s < n_rep)
        def _():
            gather_copy(which, z + s, gather_down, z).wait_recv()

            @pl.when(z > 0)
            def _():
                gather_copy(which, z + s, gather_down, z - 1).start()

    def column_copy(dz, dt):
        return remote(
            column_parts.at[z, t], column_parts.at[z, t],
            column_ssem.at[dz, dt], column_rsem.at[dz, dt],
            (shifted(z, dz, n_rep), f, shifted(t, dt, 2)),
        )

    def column_arrival(dz, dt):
        at_z, at_t = shifted(z, n_rep - dz, n_rep), shifted(t, dt, 2)
        return remote(
            column_parts.at[z, t], column_parts.at[at_z, at_t],
            column_ssem.at[dz, dt], column_rsem.at[dz, dt],
            (shifted(z, dz, n_rep), f, shifted(t, dt, 2)),
        )

    def row_power_copy(dz, df):
        return remote(
            row_parts.at[z, f], row_parts.at[z, f], row_ssem.at[dz, df], row_rsem.at[dz, df],
            (shifted(z, dz, n_rep), shifted(f, df, n_fs), t),
        )

    def row_power_arrival(dz, df):
        at_z, at_f = shifted(z, n_rep - dz, n_rep), shifted(f, n_fs - df, n_fs)
        return remote(
            row_parts.at[z, f], row_parts.at[at_z, at_f], row_ssem.at[dz, df],
            row_rsem.at[dz, df], (shifted(z, dz, n_rep), shifted(f, df, n_fs), t),
        )

    column_peers = [(dz, dt) for dz in range(n_rep) for dt in range(2) if dz or dt]
    row_peers = [(dz, df) for dz in range(n_rep) for df in range(n_fs) if dz or df]

    own_sum(GATE)
    pass_sums(UP)
    relay(GATE, 1)
    pass_sums(DOWN)
    own_sum(UP)
    for peer in column_peers:
        column_copy(*peer).start()
    for s in range(2, n_rep):
        relay(GATE, s)
    relay(UP, 1)
    own_sum(DOWN)
    for peer in row_peers:
        row_power_copy(*peer).start()
    for s in range(2, n_rep):
        relay(UP, s)
    for s in range(1, n_rep):
        relay(DOWN, s)

    grad_normed = normed_part[z, t]
    for d in range(1, n_rep):
        rep_copy(d).wait_recv()
        grad_normed = grad_normed + rep_part[d]
    normed_exact, recip_norm = normalise()
    inner = jnp.sum(grad_normed * normed_exact, axis=1, keepdims=True) * (1.0 / width)
    input_ref[...] = (recip_norm * (grad_normed - normed_exact * inner)).astype(jnp.bfloat16)

    for peer in column_peers:
        column_arrival(*peer).wait_recv()
    for peer in row_peers:
        row_power_arrival(*peer).wait_recv()
    column_power[...] = jnp.sum(column_parts[...].reshape((2 * n_rep,) + column_parts.shape[2:]), axis=0)
    row_power[...] = jnp.sum(row_parts[...], axis=1)

    for which in (GATE, UP, DOWN):
        for side in (0, 1):
            weight_copy(which, side).wait_send()
            weight_forward(which, side).wait_send()
            scatter_copy(which, side, 0).wait_send()
            scatter_copy(which, side, 1).wait_send()
            pass_copy(which, side).wait_send()
    for j in range(n_rep):
        pair_copy(j, t).wait_send()
        partner_copy(j).wait_send()

        @pl.when((z < n_rep - 1) & (z >= j))
        def _():
            row_copy(j, rows_up, z).wait_send()
            for which in (GATE, UP, DOWN):
                gather_copy(which, j, gather_up, z).wait_send()

        @pl.when((z > 0) & (z <= j))
        def _():
            row_copy(j, rows_down, z).wait_send()
            for which in (GATE, UP, DOWN):
                gather_copy(which, j, gather_down, z).wait_send()
    for d in range(1, n_rep):
        rep_copy(d).wait_send()
    for peer in column_peers:
        column_copy(*peer).wait_send()
    for peer in row_peers:
        row_power_copy(*peer).wait_send()


def assemble_kernel(
    n_rep, width,
    gate_low, gate_high, up_low, up_high, down_low, down_high, column_power, row_power,
    gate_out, up_out, down_out, gate_power, up_power, down_power,
):
    cut, units = gate_low.shape[1:]
    down_cut = down_low.shape[1]
    for j in range(n_rep):
        at = slice(j * units, (j + 1) * units)
        for low, high, out in ((gate_low, gate_high, gate_out), (up_low, up_high, up_out)):
            out[:cut, at] = low[j].astype(jnp.float32)
            out[cut:, at] = high[j]
        down_out[j * units : j * units + down_cut, :] = down_low[j].astype(jnp.float32)
        down_out[j * units + down_cut : (j + 1) * units, :] = down_high[j]
        down_power[:, at] = row_power[j, 0:1] * (1.0 / width)
    gate_power[...] = column_power[0, 0:1] * (1.0 / (2 * n_rep * units))
    up_power[...] = column_power[1, 0:1] * (1.0 / (2 * n_rep * units))


def on_device_fused(n_rep, n_fs, tokens, cotangent, gate_weight, up_weight, down_weight):
    local, width = tokens.shape
    block, hidden_local = gate_weight.shape
    units = hidden_local // n_rep
    factor = 1.0 / math.sqrt(local * 2 * n_rep * n_fs)
    count = n_rep * 2 * local
    cut, down_cut = block * 3 // 4 // 16 * 16, units * 3 // 4 // 16 * 16
    f32, bf16 = jnp.float32, jnp.bfloat16
    shapes = (
        jax.ShapeDtypeStruct((local, width), bf16),
        jax.ShapeDtypeStruct((n_rep, cut, units), bf16),
        jax.ShapeDtypeStruct((n_rep, block - cut, units), f32),
        jax.ShapeDtypeStruct((n_rep, cut, units), bf16),
        jax.ShapeDtypeStruct((n_rep, block - cut, units), f32),
        jax.ShapeDtypeStruct((n_rep, down_cut, block), bf16),
        jax.ShapeDtypeStruct((n_rep, units - down_cut, block), f32),
        jax.ShapeDtypeStruct((2, 8, block), f32),
        jax.ShapeDtypeStruct((n_rep, 8, units), f32),
    )
    dma = pltpu.SemaphoreType.DMA
    vmem = pltpu.VMEM
    scratch = [
        vmem((n_rep, 2, 2, local, width), bf16),
        vmem((n_fs, block, units), bf16),
        vmem((n_fs, block, units), bf16),
        vmem((n_fs, units, block), bf16),
        vmem((count, units), bf16),
        vmem((count, units), bf16),
        vmem((count, units), bf16),
        vmem((n_rep, 2, local, width), f32),
        vmem((n_rep, local, width), f32),
        vmem((n_rep, local, width), f32),
        vmem((n_fs, block, units), f32),
        vmem((n_fs, block, units), f32),
        vmem((n_fs, units, block), f32),
        vmem((n_fs, block, units), f32),
        vmem((n_fs, block, units), f32),
        vmem((n_fs, units, block), f32),
        vmem((n_rep, 2, 2, 8, block), f32),
        vmem((n_rep, n_fs, 8, units), f32),
        dma((n_rep,)), dma((n_rep,)), dma((n_rep,)), dma((n_rep,)), dma((n_rep,)),
        dma((3, 4)), dma((3, 4)),
        dma((n_rep,)), dma((n_rep,)), dma((n_rep,)), dma((n_rep,)),
        dma((3, 6)), dma((3, 6)),
        dma((3, 2, n_rep)), dma((3, 2, n_rep)), dma((3, 2, n_rep)),
        dma((n_rep, 2)), dma((n_rep, 2)), dma((n_rep, n_fs)), dma((n_rep, n_fs)),
    ]
    whole = pl.BlockSpec(memory_space=pltpu.VMEM)
    input_grad, *blocks = pl.pallas_call(
        functools.partial(exchange_kernel, n_rep, n_fs, factor),
        out_shape=shapes,
        in_specs=[whole] * 5,
        out_specs=(whole,) * 9,
        scratch_shapes=scratch,
        compiler_params=pltpu.CompilerParams(
            collective_id=0, has_side_effects=True, vmem_limit_bytes=63 * 1024 * 1024
        ),
    )(tokens, cotangent, gate_weight, up_weight, down_weight)
    gate_grad, up_grad, down_grad, gate_power, up_power, down_power = pl.pallas_call(
        functools.partial(assemble_kernel, n_rep, width),
        out_shape=(
            jax.ShapeDtypeStruct((block, hidden_local), f32),
            jax.ShapeDtypeStruct((block, hidden_local), f32),
            jax.ShapeDtypeStruct((hidden_local, block), f32),
            jax.ShapeDtypeStruct((1, block), f32),
            jax.ShapeDtypeStruct((1, block), f32),
            jax.ShapeDtypeStruct((1, hidden_local), f32),
        ),
        in_specs=[whole] * 8,
        out_specs=(whole,) * 6,
        compiler_params=pltpu.CompilerParams(vmem_limit_bytes=63 * 1024 * 1024),
    )(*blocks)
    return (
        input_grad, gate_grad, up_grad, down_grad,
        gate_power.reshape(block), up_power.reshape(block), down_power.reshape(hidden_local),
    )


def solution(mesh):
    placed = (
        P(("rep", "fs", "tp"), None),
        P(("rep", "fs", "tp"), None),
        P("fs", "tp"),
        P("fs", "tp"),
        P("tp", "fs"),
    )
    n_rep, n_fs = mesh.shape["rep"], mesh.shape["fs"]
    step = on_device
    if mesh.shape["tp"] == 2 and n_fs == 4 and FF // 2 % (16 * n_rep) == 0 and D % (128 * n_fs) == 0:
        step = functools.partial(on_device_fused, n_rep, n_fs)
    return jax.shard_map(
        step,
        mesh=mesh,
        in_specs=placed,
        out_specs=(
            P(("rep", "fs", "tp"), None),
            P("fs", "tp"),
            P("fs", "tp"),
            P("tp", "fs"),
            P("fs"),
            P("fs"),
            P("tp"),
        ),
        check_vma=False,
    )
```

```python
import functools
import math

import jax
import jax.numpy as jnp
from jax import lax
from jax.experimental import pallas as pl
from jax.experimental.pallas import tpu as pltpu
from jax.sharding import PartitionSpec as P

D = 1024
FF = 2816


EPSILON = 1e-06


def contract_rows(left, right):
    return lax.dot_general(
        left, right, (((0,), (0,)), ((), ())), preferred_element_type=jnp.float32
    )


def contract_cols(left, right):
    return lax.dot_general(
        left, right, (((1,), (1,)), ((), ())), preferred_element_type=jnp.float32
    )


def on_device(tokens, cotangent, gate_weight, up_weight, down_weight):
    tp_count = lax.axis_size("tp")
    fs_count = lax.axis_size("fs")
    rep_count = lax.axis_size("rep")
    width = tokens.shape[1]
    factor = 1.0 / math.sqrt(tokens.shape[0] * tp_count * fs_count * rep_count)
    xfloat = tokens.astype(jnp.float32)
    recip_norm = lax.rsqrt(jnp.mean(xfloat * xfloat, axis=1, keepdims=True) + EPSILON)
    normed_exact = xfloat * recip_norm
    normed = normed_exact.astype(jnp.bfloat16)
    group_normed, group_cotangent = (
        lax.all_gather(normed, "tp", axis=0, tiled=True),
        lax.all_gather(cotangent, "tp", axis=0, tiled=True),
    )
    gate_full, up_full, down_full = (
        lax.all_gather(gate_weight, "fs", axis=0, tiled=True),
        lax.all_gather(up_weight, "fs", axis=0, tiled=True),
        lax.all_gather(down_weight.T, "fs", axis=0, tiled=True),
    )
    gate_pre = jnp.dot(group_normed, gate_full, preferred_element_type=jnp.float32)
    up_pre = jnp.dot(group_normed, up_full, preferred_element_type=jnp.float32)
    sigmoid_gate = jax.nn.sigmoid(gate_pre)
    activated = gate_pre * sigmoid_gate
    hidden = (activated * up_pre).astype(jnp.bfloat16)
    grad_hidden = 0.5 * jnp.dot(group_cotangent, down_full, preferred_element_type=jnp.float32)
    grad_up_pre = (grad_hidden * activated).astype(jnp.bfloat16)
    grad_gate_pre = (
        grad_hidden * up_pre * sigmoid_gate * (1.0 + gate_pre * (1.0 - sigmoid_gate))
    ).astype(jnp.bfloat16)
    normed_part = contract_cols(grad_gate_pre, gate_full) + contract_cols(grad_up_pre, up_full)
    grad_normed = lax.psum_scatter(normed_part, "tp", scatter_dimension=0, tiled=True)
    inner = jnp.mean(grad_normed * normed_exact, axis=1, keepdims=True)
    input_grad = (recip_norm * (grad_normed - normed_exact * inner)).astype(jnp.bfloat16)
    hidden_local = gate_weight.shape[1]

    def rows_term():
        normed_cols = lax.slice_in_dim(
            group_normed, 0, width // fs_count * lax.axis_size("fs"), axis=1
        )
        cotangent_cols = lax.slice_in_dim(
            group_cotangent, 0, width // fs_count * lax.axis_size("fs"), axis=1
        )
        return factor * jnp.concatenate(
            [
                contract_rows(normed_cols, grad_gate_pre),
                contract_rows(normed_cols, grad_up_pre),
                0.5 * contract_rows(cotangent_cols, hidden),
            ],
            axis=1,
        )

    reduced = lax.psum_scatter(rows_term(), "fs", scatter_dimension=0, tiled=True)
    reduced = lax.psum(reduced, "rep")
    gate_grad = reduced[:, :hidden_local]
    up_grad = reduced[:, hidden_local : 2 * hidden_local]
    down_grad = reduced[:, 2 * hidden_local :].T
    gate_sums, up_sums = lax.psum(
        (jnp.sum(gate_grad * gate_grad, axis=1), jnp.sum(up_grad * up_grad, axis=1)), "tp"
    )
    down_sums = lax.psum(jnp.sum(down_grad * down_grad, axis=1), "fs")
    return (input_grad, gate_grad, up_grad, down_grad, gate_sums / FF, up_sums / FF, down_sums / D)


MESH = pl.DeviceIdType.MESH
GATE, UP, DOWN = 0, 1, 2


def exchange_kernel(
    n_rep, n_fs, factor,
    tokens_ref, cotangent_ref, gate_ref, up_ref, down_ref,
    input_ref, gate_low, gate_high, up_low, up_high, down_low, down_high, column_power, row_power,
    rows_all, gate_all, up_all, down_all,
    grad_gate, grad_up, hidden_all,
    normed_part, partner_part, rep_part,
    gate_send, up_send, down_send, gate_recv, up_recv, down_recv,
    column_parts, row_parts,
    rows_up, rows_down, rows_recv, pair_send, pair_recv,
    weight_ssem, weight_rsem,
    partner_ssem, partner_rsem, rep_ssem, rep_rsem,
    scatter_ssem, scatter_rsem,
    gather_up, gather_down, gather_rsem,
    column_ssem, column_rsem, row_ssem, row_rsem,
):
    z, f, t = lax.axis_index("rep"), lax.axis_index("fs"), lax.axis_index("tp")
    other = 1 - t
    side_x = f + 1 - 2 * lax.rem(f, 2)
    side_y = lax.rem(f + 2, n_fs)
    across = lax.rem(side_x + 2, n_fs)
    sides = (side_x, side_y)
    local, width = tokens_ref.shape
    block = gate_ref.shape[0]
    hidden_units = gate_all.shape[2]
    chunk = 2 * local

    def remote(source, target, send_sem, recv_sem, where):
        return pltpu.make_async_remote_copy(
            src_ref=source, dst_ref=target, send_sem=send_sem, recv_sem=recv_sem,
            device_id={"rep": where[0], "fs": where[1], "tp": where[2]},
            device_id_type=MESH,
        )

    def shifted(value, by, count):
        return lax.rem(value + by, count)

    barrier = pltpu.get_barrier_semaphore()

    def greet(where):
        pl.semaphore_signal(
            barrier, inc=1, device_id={"rep": where[0], "fs": where[1], "tp": where[2]},
            device_id_type=MESH,
        )

    for dz in range(n_rep):
        for df in range(n_fs):
            if dz or df:
                greet((shifted(z, dz, n_rep), shifted(f, df, n_fs), t))
        greet((shifted(z, dz, n_rep), f, other))

    def normalise():
        xfloat = tokens_ref[...].astype(jnp.float32)
        mean = jnp.sum(xfloat * xfloat, axis=1, keepdims=True) * (1.0 / width)
        recip_norm = lax.rsqrt(mean + EPSILON)
        return xfloat * recip_norm, recip_norm

    rows_all[z, t, 0] = normalise()[0].astype(jnp.bfloat16)
    rows_all[z, t, 1] = cotangent_ref[...]
    for j in range(n_rep):
        @pl.when(z == j)
        def _():
            gate_all[f] = gate_ref[:, j * hidden_units : (j + 1) * hidden_units]
            up_all[f] = up_ref[:, j * hidden_units : (j + 1) * hidden_units]

    units_at = pl.ds(pl.multiple_of(z * hidden_units, 16), hidden_units)
    down_all[f] = down_ref[units_at, :]
    pl.semaphore_wait(barrier, n_rep * n_fs - 1 + n_rep)

    weights = ((gate_all.at[f], gate_all), (up_all.at[f], up_all), (down_ref.at[units_at], down_all))

    def weight_copy(which, side):
        source, target = weights[which]
        return remote(
            source, target.at[f], weight_ssem.at[which, side], weight_rsem.at[which, side],
            (z, sides[side], t),
        )

    def weight_arrival(which, side):
        target = weights[which][1].at[sides[side]]
        return remote(
            target, target, weight_ssem.at[which, side], weight_rsem.at[which, side],
            (z, sides[side], t),
        )

    def half_of(which, part):
        rows = weights[which][1].shape[1] // 2
        return pl.ds(part * rows, rows)

    def weight_forward(which, side):
        origin = sides[1 - side]
        part = weights[which][1].at[origin, half_of(which, 1 - side)]
        return remote(
            part, part, weight_ssem.at[which, 2 + side], weight_rsem.at[which, 2 + side],
            (z, sides[side], t),
        )

    def weight_across(which, side):
        part = weights[which][1].at[across, half_of(which, 1 - side)]
        return remote(
            part, part, weight_ssem.at[which, 2 + side], weight_rsem.at[which, 2 + side],
            (z, sides[side], t),
        )

    def pass_weights(which):
        for side in (0, 1):
            weight_arrival(which, side).wait_recv()
            weight_forward(which, 1 - side).start()

    def row_copy(j, sems, to):
        return remote(
            rows_all.at[j, t], rows_all.at[j, t], sems.at[j], rows_recv.at[j], (to, f, t)
        )

    def pair_copy(j, half):
        return remote(
            rows_all.at[j, half], rows_all.at[j, half], pair_send.at[j], pair_recv.at[j],
            (z, f, other),
        )

    @pl.when(z < n_rep - 1)
    def _():
        row_copy(z, rows_up, z + 1).start()

    @pl.when(z > 0)
    def _():
        row_copy(z, rows_down, z - 1).start()

    for which in (GATE, UP, DOWN):
        for side in (0, 1):
            weight_copy(which, side).start()
    pair_copy(z, t).start()

    for s in range(1, max(n_rep, 4)):
        if s <= 3:
            pass_weights(s - 1)
        if s >= n_rep:
            continue

        @pl.when(z - s >= 0)
        def _():
            row_copy(z - s, rows_up, z).wait_recv()
            pair_copy(z - s, t).start()

            @pl.when(z < n_rep - 1)
            def _():
                row_copy(z - s, rows_up, z + 1).start()

        @pl.when(z + s < n_rep)
        def _():
            row_copy(z + s, rows_down, z).wait_recv()
            pair_copy(z + s, t).start()

            @pl.when(z > 0)
            def _():
                row_copy(z + s, rows_down, z - 1).start()

    for j in range(n_rep):
        pair_copy(j, other).wait_recv()
    for which in (GATE, UP, DOWN):
        for side in (0, 1):
            weight_across(which, side).wait_recv()

    def forward(j, carry):
        normed = rows_all[j, :, 0].reshape(chunk, width)
        cotangent = rows_all[j, :, 1].reshape(chunk, width)
        gate_pre = jnp.dot(
            normed, gate_all[...].reshape(width, hidden_units), preferred_element_type=jnp.float32
        )
        up_pre = jnp.dot(
            normed, up_all[...].reshape(width, hidden_units), preferred_element_type=jnp.float32
        )
        grad_hidden = jnp.zeros((chunk, hidden_units), jnp.float32)
        for k in range(n_fs):
            grad_hidden += contract_cols(cotangent[:, k * block : (k + 1) * block], down_all[k])
        grad_hidden = 0.5 * grad_hidden
        sigmoid_gate = jax.nn.sigmoid(gate_pre)
        activated = gate_pre * sigmoid_gate
        at = pl.ds(pl.multiple_of(j * chunk, chunk), chunk)
        hidden_all[at, :] = (activated * up_pre).astype(jnp.bfloat16)
        grad_up_pre = (grad_hidden * activated).astype(jnp.bfloat16)
        grad_gate_pre = (
            grad_hidden * up_pre * sigmoid_gate * (1.0 + gate_pre * (1.0 - sigmoid_gate))
        ).astype(jnp.bfloat16)
        grad_up[at, :] = grad_up_pre
        grad_gate[at, :] = grad_gate_pre
        return carry

    lax.fori_loop(0, n_rep, forward, 0)

    def backward(j, carry):
        at = pl.ds(pl.multiple_of(j * chunk, chunk), chunk)
        for k in range(n_fs):
            part = contract_cols(grad_gate[at, :], gate_all[k]) + contract_cols(
                grad_up[at, :], up_all[k]
            )
            normed_part[j, :, :, k * block : (k + 1) * block] = part.reshape(2, local, block)
        return carry

    def partner_copy(j):
        return remote(
            normed_part.at[j, other], partner_part.at[j], partner_ssem.at[j], partner_rsem.at[j],
            (z, f, other),
        )

    def columns_of(half, k):
        at = pl.ds(pl.multiple_of(k * block, block), block)
        return rows_all[:, :, half, :, at].reshape(n_rep * chunk, block)

    def term(which, k):
        if which == GATE:
            return contract_rows(columns_of(0, k), grad_gate[...])
        if which == UP:
            return contract_rows(columns_of(0, k), grad_up[...])
        return contract_rows(hidden_all[...], columns_of(1, k))

    sums = ((gate_send, gate_recv), (up_send, up_recv), (down_send, down_recv))

    def half(which, part):
        rows = sums[which][0].shape[1] // 2
        return pl.ds(part * rows, rows)

    def scatter_copy(which, side, kind):
        source, target = sums[which]
        at = half(which, side)
        slot = (1 + side) if kind == 0 else 3
        sem = 2 * side + kind
        return remote(
            source.at[slot, at], target.at[kind, at],
            scatter_ssem.at[which, sem], scatter_rsem.at[which, sem], (z, sides[side], t),
        )

    def pass_copy(which, side):
        source, target = sums[which]
        at = half(which, 1 - side)
        return remote(
            source.at[1 + side, at], target.at[2, at],
            scatter_ssem.at[which, 4 + side], scatter_rsem.at[which, 4 + side],
            (z, sides[side], t),
        )

    def send_terms(which):
        sums[which][0][3] = term(which, across)
        for side in (0, 1):
            scatter_copy(which, side, 1).start()
        for side in (0, 1):
            sums[which][0][1 + side] = term(which, sides[side])
            scatter_copy(which, side, 0).start()

    def pass_sums(which):
        source, target = sums[which]
        for side in (0, 1):
            scatter_copy(which, 1 - side, 1).wait_recv()
            at = half(which, 1 - side)
            source[1 + side, at] = source[1 + side, at] + target[1, at]
            pass_copy(which, side).start()

    def rep_copy(d):
        return remote(
            normed_part.at[shifted(z, d, n_rep), t], rep_part.at[d],
            rep_ssem.at[d], rep_rsem.at[d], (shifted(z, d, n_rep), f, t),
        )

    send_terms(GATE)
    lax.fori_loop(0, n_rep, backward, 0)
    for j in range(n_rep):
        partner_copy(j).start()
    send_terms(UP)
    for j in range(n_rep):
        partner_copy(j).wait_recv()
        normed_part[j, t] = normed_part[j, t] + partner_part[j]
    for d in range(1, n_rep):
        rep_copy(d).start()
    sums[GATE][0][0] = term(GATE, f)
    pass_sums(GATE)
    send_terms(DOWN)
    for which in (UP, DOWN):
        sums[which][0][0] = term(which, f)

    outs = ((gate_low, gate_high), (up_low, up_high), (down_low, down_high))

    class gather_copy:
        def __init__(self, which, j, sems, to):
            self.pieces = [
                remote(
                    out.at[j], out.at[j], sems.at[which, part, j],
                    gather_rsem.at[which, part, j], (to, f, t),
                )
                for part, out in enumerate(outs[which])
            ]

        def start(self):
            for piece in self.pieces:
                piece.start()

        def wait_recv(self):
            for piece in self.pieces:
                piece.wait_recv()

        def wait_send(self):
            for piece in self.pieces:
                piece.wait_send()

    def row_squares(value):
        return lax.dot_general(
            jnp.ones((8, value.shape[1]), jnp.float32), value * value,
            (((1,), (1,)), ((), ())), preferred_element_type=jnp.float32,
            precision=lax.Precision.HIGHEST,
        )

    def own_sum(which):
        source, target = sums[which]
        for side in (0, 1):
            scatter_copy(which, side, 0).wait_recv()
            pass_copy(which, side).wait_recv()
        total = source[0] + target[0] + target[2]
        total = total * (factor if which != DOWN else 0.5 * factor)
        cut = outs[which][0].shape[1]
        outs[which][0][z] = total[:cut].astype(jnp.bfloat16)
        outs[which][1][z] = total[cut:]

        @pl.when(z < n_rep - 1)
        def _():
            gather_copy(which, z, gather_up, z + 1).start()

        @pl.when(z > 0)
        def _():
            gather_copy(which, z, gather_down, z - 1).start()

        if which == DOWN:
            row_parts[z, f] = row_squares(total)
        else:
            column_parts[z, t, which] = row_squares(total)

    def relay(which, s):
        @pl.when((z - s >= 0) & (z < n_rep - 1))
        def _():
            gather_copy(which, z - s, gather_up, z).wait_recv()
            gather_copy(which, z - s, gather_up, z + 1).start()

        @pl.when((z + s < n_rep) & (z > 0))
        def _():
            gather_copy(which, z + s, gather_down, z).wait_recv()
            gather_copy(which, z + s, gather_down, z - 1).start()

    def collect(which, s):
        @pl.when((z - s >= 0) & (z == n_rep - 1))
        def _():
            gather_copy(which, z - s, gather_up, z).wait_recv()

        @pl.when((z + s < n_rep) & (z == 0))
        def _():
            gather_copy(which, z + s, gather_down, z).wait_recv()

    def column_copy(dz, dt):
        return remote(
            column_parts.at[z, t], column_parts.at[z, t],
            column_ssem.at[dz, dt], column_rsem.at[dz, dt],
            (shifted(z, dz, n_rep), f, shifted(t, dt, 2)),
        )

    def column_arrival(dz, dt):
        at_z, at_t = shifted(z, n_rep - dz, n_rep), shifted(t, dt, 2)
        return remote(
            column_parts.at[z, t], column_parts.at[at_z, at_t],
            column_ssem.at[dz, dt], column_rsem.at[dz, dt],
            (shifted(z, dz, n_rep), f, shifted(t, dt, 2)),
        )

    def row_power_copy(dz, df):
        return remote(
            row_parts.at[z, f], row_parts.at[z, f], row_ssem.at[dz, df], row_rsem.at[dz, df],
            (shifted(z, dz, n_rep), shifted(f, df, n_fs), t),
        )

    def row_power_arrival(dz, df):
        at_z, at_f = shifted(z, n_rep - dz, n_rep), shifted(f, n_fs - df, n_fs)
        return remote(
            row_parts.at[z, f], row_parts.at[at_z, at_f], row_ssem.at[dz, df],
            row_rsem.at[dz, df], (shifted(z, dz, n_rep), shifted(f, df, n_fs), t),
        )

    column_peers = [(dz, dt) for dz in range(n_rep) for dt in range(2) if dz or dt]
    row_peers = [(dz, df) for dz in range(n_rep) for df in range(n_fs) if dz or df]

    own_sum(GATE)
    pass_sums(UP)
    relay(GATE, 1)
    pass_sums(DOWN)
    own_sum(UP)
    for peer in column_peers:
        column_copy(*peer).start()
    for s in range(2, n_rep - 1):
        relay(GATE, s)
    own_sum(DOWN)
    for peer in row_peers:
        row_power_copy(*peer).start()
    for s in range(1, n_rep - 1):
        relay(UP, s)
    for s in range(1, n_rep - 1):
        relay(DOWN, s)

    grad_normed = normed_part[z, t]
    for d in range(1, n_rep):
        rep_copy(d).wait_recv()
        grad_normed = grad_normed + rep_part[d]
    normed_exact, recip_norm = normalise()
    inner = jnp.sum(grad_normed * normed_exact, axis=1, keepdims=True) * (1.0 / width)
    input_ref[...] = (recip_norm * (grad_normed - normed_exact * inner)).astype(jnp.bfloat16)

    for which in (GATE, UP, DOWN):
        for s in range(1, n_rep):
            collect(which, s)
    for peer in column_peers:
        column_arrival(*peer).wait_recv()
    for peer in row_peers:
        row_power_arrival(*peer).wait_recv()
    column_power[...] = jnp.sum(column_parts[...].reshape((2 * n_rep,) + column_parts.shape[2:]), axis=0)
    row_power[...] = jnp.sum(row_parts[...], axis=1)

    for which in (GATE, UP, DOWN):
        for side in (0, 1):
            weight_copy(which, side).wait_send()
            weight_forward(which, side).wait_send()
            scatter_copy(which, side, 0).wait_send()
            scatter_copy(which, side, 1).wait_send()
            pass_copy(which, side).wait_send()
    for j in range(n_rep):
        pair_copy(j, t).wait_send()
        partner_copy(j).wait_send()

        @pl.when((z < n_rep - 1) & (z >= j))
        def _():
            row_copy(j, rows_up, z).wait_send()
            for which in (GATE, UP, DOWN):
                gather_copy(which, j, gather_up, z).wait_send()

        @pl.when((z > 0) & (z <= j))
        def _():
            row_copy(j, rows_down, z).wait_send()
            for which in (GATE, UP, DOWN):
                gather_copy(which, j, gather_down, z).wait_send()
    for d in range(1, n_rep):
        rep_copy(d).wait_send()
    for peer in column_peers:
        column_copy(*peer).wait_send()
    for peer in row_peers:
        row_power_copy(*peer).wait_send()


def assemble_kernel(
    n_rep, width,
    gate_low, gate_high, up_low, up_high, down_low, down_high, column_power, row_power,
    gate_out, up_out, down_out, gate_power, up_power, down_power,
):
    cut, units = gate_low.shape[1:]
    down_cut = down_low.shape[1]
    for j in range(n_rep):
        at = slice(j * units, (j + 1) * units)
        for low, high, out in ((gate_low, gate_high, gate_out), (up_low, up_high, up_out)):
            out[:cut, at] = low[j].astype(jnp.float32)
            out[cut:, at] = high[j]
        down_out[j * units : j * units + down_cut, :] = down_low[j].astype(jnp.float32)
        down_out[j * units + down_cut : (j + 1) * units, :] = down_high[j]
        down_power[:, at] = row_power[j, 0:1] * (1.0 / width)
    gate_power[...] = column_power[0, 0:1] * (1.0 / (2 * n_rep * units))
    up_power[...] = column_power[1, 0:1] * (1.0 / (2 * n_rep * units))


def on_device_fused(n_rep, n_fs, tokens, cotangent, gate_weight, up_weight, down_weight):
    local, width = tokens.shape
    block, hidden_local = gate_weight.shape
    units = hidden_local // n_rep
    factor = 1.0 / math.sqrt(local * 2 * n_rep * n_fs)
    count = n_rep * 2 * local
    cut, down_cut = block * 3 // 4 // 16 * 16, units * 3 // 4 // 16 * 16
    f32, bf16 = jnp.float32, jnp.bfloat16
    shapes = (
        jax.ShapeDtypeStruct((local, width), bf16),
        jax.ShapeDtypeStruct((n_rep, cut, units), bf16),
        jax.ShapeDtypeStruct((n_rep, block - cut, units), f32),
        jax.ShapeDtypeStruct((n_rep, cut, units), bf16),
        jax.ShapeDtypeStruct((n_rep, block - cut, units), f32),
        jax.ShapeDtypeStruct((n_rep, down_cut, block), bf16),
        jax.ShapeDtypeStruct((n_rep, units - down_cut, block), f32),
        jax.ShapeDtypeStruct((2, 8, block), f32),
        jax.ShapeDtypeStruct((n_rep, 8, units), f32),
    )
    dma = pltpu.SemaphoreType.DMA
    vmem = pltpu.VMEM
    scratch = [
        vmem((n_rep, 2, 2, local, width), bf16),
        vmem((n_fs, block, units), bf16),
        vmem((n_fs, block, units), bf16),
        vmem((n_fs, units, block), bf16),
        vmem((count, units), bf16),
        vmem((count, units), bf16),
        vmem((count, units), bf16),
        vmem((n_rep, 2, local, width), f32),
        vmem((n_rep, local, width), f32),
        vmem((n_rep, local, width), f32),
        vmem((n_fs, block, units), f32),
        vmem((n_fs, block, units), f32),
        vmem((n_fs, units, block), f32),
        vmem((n_fs, block, units), f32),
        vmem((n_fs, block, units), f32),
        vmem((n_fs, units, block), f32),
        vmem((n_rep, 2, 2, 8, block), f32),
        vmem((n_rep, n_fs, 8, units), f32),
        dma((n_rep,)), dma((n_rep,)), dma((n_rep,)), dma((n_rep,)), dma((n_rep,)),
        dma((3, 4)), dma((3, 4)),
        dma((n_rep,)), dma((n_rep,)), dma((n_rep,)), dma((n_rep,)),
        dma((3, 6)), dma((3, 6)),
        dma((3, 2, n_rep)), dma((3, 2, n_rep)), dma((3, 2, n_rep)),
        dma((n_rep, 2)), dma((n_rep, 2)), dma((n_rep, n_fs)), dma((n_rep, n_fs)),
    ]
    whole = pl.BlockSpec(memory_space=pltpu.VMEM)
    input_grad, *blocks = pl.pallas_call(
        functools.partial(exchange_kernel, n_rep, n_fs, factor),
        out_shape=shapes,
        in_specs=[whole] * 5,
        out_specs=(whole,) * 9,
        scratch_shapes=scratch,
        compiler_params=pltpu.CompilerParams(
            collective_id=0, has_side_effects=True, vmem_limit_bytes=63 * 1024 * 1024
        ),
    )(tokens, cotangent, gate_weight, up_weight, down_weight)
    gate_grad, up_grad, down_grad, gate_power, up_power, down_power = pl.pallas_call(
        functools.partial(assemble_kernel, n_rep, width),
        out_shape=(
            jax.ShapeDtypeStruct((block, hidden_local), f32),
            jax.ShapeDtypeStruct((block, hidden_local), f32),
            jax.ShapeDtypeStruct((hidden_local, block), f32),
            jax.ShapeDtypeStruct((1, block), f32),
            jax.ShapeDtypeStruct((1, block), f32),
            jax.ShapeDtypeStruct((1, hidden_local), f32),
        ),
        in_specs=[whole] * 8,
        out_specs=(whole,) * 6,
        compiler_params=pltpu.CompilerParams(vmem_limit_bytes=63 * 1024 * 1024),
    )(*blocks)
    return (
        input_grad, gate_grad, up_grad, down_grad,
        gate_power.reshape(block), up_power.reshape(block), down_power.reshape(hidden_local),
    )


def solution(mesh):
    placed = (
        P(("rep", "fs", "tp"), None),
        P(("rep", "fs", "tp"), None),
        P("fs", "tp"),
        P("fs", "tp"),
        P("tp", "fs"),
    )
    n_rep, n_fs = mesh.shape["rep"], mesh.shape["fs"]

    def step(tokens, cotangent, gate_weight, up_weight, down_weight):
        block, hidden_local = gate_weight.shape
        run = on_device
        if mesh.shape["tp"] == 2 and n_fs == 4:
            if hidden_local % (16 * n_rep) == 0 and block % 128 == 0:
                run = functools.partial(on_device_fused, n_rep, n_fs)
        return run(tokens, cotangent, gate_weight, up_weight, down_weight)

    return jax.shard_map(
        step,
        mesh=mesh,
        in_specs=placed,
        out_specs=(
            P(("rep", "fs", "tp"), None),
            P("fs", "tp"),
            P("fs", "tp"),
            P("tp", "fs"),
            P("fs"),
            P("fs"),
            P("tp"),
        ),
        check_vma=False,
    )
```

```python
import functools
import math

import jax
import jax.numpy as jnp
from jax import lax
from jax.experimental import pallas as pl
from jax.experimental.pallas import tpu as pltpu
from jax.sharding import PartitionSpec as P

D = 1024
FF = 2816


EPSILON = 1e-06


def contract_rows(left, right):
    return lax.dot_general(
        left, right, (((0,), (0,)), ((), ())), preferred_element_type=jnp.float32
    )


def contract_cols(left, right):
    return lax.dot_general(
        left, right, (((1,), (1,)), ((), ())), preferred_element_type=jnp.float32
    )


def on_device(tokens, cotangent, gate_weight, up_weight, down_weight):
    tp_count = lax.axis_size("tp")
    fs_count = lax.axis_size("fs")
    rep_count = lax.axis_size("rep")
    width = tokens.shape[1]
    factor = 1.0 / math.sqrt(tokens.shape[0] * tp_count * fs_count * rep_count)
    xfloat = tokens.astype(jnp.float32)
    recip_norm = lax.rsqrt(jnp.mean(xfloat * xfloat, axis=1, keepdims=True) + EPSILON)
    normed_exact = xfloat * recip_norm
    normed = normed_exact.astype(jnp.bfloat16)
    group_normed, group_cotangent = (
        lax.all_gather(normed, "tp", axis=0, tiled=True),
        lax.all_gather(cotangent, "tp", axis=0, tiled=True),
    )
    gate_full, up_full, down_full = (
        lax.all_gather(gate_weight, "fs", axis=0, tiled=True),
        lax.all_gather(up_weight, "fs", axis=0, tiled=True),
        lax.all_gather(down_weight.T, "fs", axis=0, tiled=True),
    )
    gate_pre = jnp.dot(group_normed, gate_full, preferred_element_type=jnp.float32)
    up_pre = jnp.dot(group_normed, up_full, preferred_element_type=jnp.float32)
    sigmoid_gate = jax.nn.sigmoid(gate_pre)
    activated = gate_pre * sigmoid_gate
    hidden = (activated * up_pre).astype(jnp.bfloat16)
    grad_hidden = 0.5 * jnp.dot(group_cotangent, down_full, preferred_element_type=jnp.float32)
    grad_up_pre = (grad_hidden * activated).astype(jnp.bfloat16)
    grad_gate_pre = (
        grad_hidden * up_pre * sigmoid_gate * (1.0 + gate_pre * (1.0 - sigmoid_gate))
    ).astype(jnp.bfloat16)
    normed_part = contract_cols(grad_gate_pre, gate_full) + contract_cols(grad_up_pre, up_full)
    grad_normed = lax.psum_scatter(normed_part, "tp", scatter_dimension=0, tiled=True)
    inner = jnp.mean(grad_normed * normed_exact, axis=1, keepdims=True)
    input_grad = (recip_norm * (grad_normed - normed_exact * inner)).astype(jnp.bfloat16)
    hidden_local = gate_weight.shape[1]

    def rows_term():
        normed_cols = lax.slice_in_dim(
            group_normed, 0, width // fs_count * lax.axis_size("fs"), axis=1
        )
        cotangent_cols = lax.slice_in_dim(
            group_cotangent, 0, width // fs_count * lax.axis_size("fs"), axis=1
        )
        return factor * jnp.concatenate(
            [
                contract_rows(normed_cols, grad_gate_pre),
                contract_rows(normed_cols, grad_up_pre),
                0.5 * contract_rows(cotangent_cols, hidden),
            ],
            axis=1,
        )

    reduced = lax.psum_scatter(rows_term(), "fs", scatter_dimension=0, tiled=True)
    reduced = lax.psum(reduced, "rep")
    gate_grad = reduced[:, :hidden_local]
    up_grad = reduced[:, hidden_local : 2 * hidden_local]
    down_grad = reduced[:, 2 * hidden_local :].T
    gate_sums, up_sums = lax.psum(
        (jnp.sum(gate_grad * gate_grad, axis=1), jnp.sum(up_grad * up_grad, axis=1)), "tp"
    )
    down_sums = lax.psum(jnp.sum(down_grad * down_grad, axis=1), "fs")
    return (input_grad, gate_grad, up_grad, down_grad, gate_sums / FF, up_sums / FF, down_sums / D)


MESH = pl.DeviceIdType.MESH
GATE, UP, DOWN = 0, 1, 2


def exchange_kernel(
    n_rep, n_fs, factor,
    tokens_ref, cotangent_ref, gate_ref, up_ref, down_ref,
    input_ref, gate_low, gate_high, up_low, up_high, down_low, down_high, column_power, row_power,
    rows_all, gate_all, up_all, down_all,
    grad_gate, grad_up, hidden_all,
    normed_part, partner_part, rep_part,
    gate_send, up_send, down_send, gate_recv, up_recv, down_recv,
    column_parts, row_parts,
    rows_up, rows_down, rows_recv, pair_send, pair_recv,
    weight_ssem, weight_rsem,
    partner_ssem, partner_rsem, rep_ssem, rep_rsem,
    scatter_ssem, scatter_rsem,
    gather_up, gather_down, gather_rsem,
    column_ssem, column_rsem, row_ssem, row_rsem,
):
    z, f, t = lax.axis_index("rep"), lax.axis_index("fs"), lax.axis_index("tp")
    other = 1 - t
    side_x = f + 1 - 2 * lax.rem(f, 2)
    side_y = lax.rem(f + 2, n_fs)
    across = lax.rem(side_x + 2, n_fs)
    sides = (side_x, side_y)
    local, width = tokens_ref.shape
    block = gate_ref.shape[0]
    hidden_units = gate_all.shape[2]
    chunk = 2 * local

    def remote(source, target, send_sem, recv_sem, where):
        return pltpu.make_async_remote_copy(
            src_ref=source, dst_ref=target, send_sem=send_sem, recv_sem=recv_sem,
            device_id={"rep": where[0], "fs": where[1], "tp": where[2]},
            device_id_type=MESH,
        )

    def shifted(value, by, count):
        return lax.rem(value + by, count)

    barrier = pltpu.get_barrier_semaphore()

    def greet(where):
        pl.semaphore_signal(
            barrier, inc=1, device_id={"rep": where[0], "fs": where[1], "tp": where[2]},
            device_id_type=MESH,
        )

    for dz in range(n_rep):
        for df in range(n_fs):
            if dz or df:
                greet((shifted(z, dz, n_rep), shifted(f, df, n_fs), t))
        greet((shifted(z, dz, n_rep), f, other))

    def normalise():
        xfloat = tokens_ref[...].astype(jnp.float32)
        mean = jnp.sum(xfloat * xfloat, axis=1, keepdims=True) * (1.0 / width)
        recip_norm = lax.rsqrt(mean + EPSILON)
        return xfloat * recip_norm, recip_norm

    rows_all[z, t, 0] = normalise()[0].astype(jnp.bfloat16)
    rows_all[z, t, 1] = cotangent_ref[...]
    for j in range(n_rep):
        @pl.when(z == j)
        def _():
            gate_all[f] = gate_ref[:, j * hidden_units : (j + 1) * hidden_units]
            up_all[f] = up_ref[:, j * hidden_units : (j + 1) * hidden_units]

    units_at = pl.ds(pl.multiple_of(z * hidden_units, 16), hidden_units)
    down_all[f] = down_ref[units_at, :]
    pl.semaphore_wait(barrier, n_rep * n_fs - 1 + n_rep)

    weights = ((gate_all.at[f], gate_all), (up_all.at[f], up_all), (down_ref.at[units_at], down_all))

    def weight_copy(which, side):
        source, target = weights[which]
        return remote(
            source, target.at[f], weight_ssem.at[which, side], weight_rsem.at[which, side],
            (z, sides[side], t),
        )

    def weight_arrival(which, side):
        target = weights[which][1].at[sides[side]]
        return remote(
            target, target, weight_ssem.at[which, side], weight_rsem.at[which, side],
            (z, sides[side], t),
        )

    def half_of(which, part):
        rows = weights[which][1].shape[1] // 2
        return pl.ds(part * rows, rows)

    def weight_forward(which, side):
        origin = sides[1 - side]
        part = weights[which][1].at[origin, half_of(which, 1 - side)]
        return remote(
            part, part, weight_ssem.at[which, 2 + side], weight_rsem.at[which, 2 + side],
            (z, sides[side], t),
        )

    def weight_across(which, side):
        part = weights[which][1].at[across, half_of(which, 1 - side)]
        return remote(
            part, part, weight_ssem.at[which, 2 + side], weight_rsem.at[which, 2 + side],
            (z, sides[side], t),
        )

    def pass_weights(which):
        for side in (0, 1):
            weight_arrival(which, side).wait_recv()
            weight_forward(which, 1 - side).start()

    def row_copy(j, sems, to):
        return remote(
            rows_all.at[j, t], rows_all.at[j, t], sems.at[j], rows_recv.at[j], (to, f, t)
        )

    def pair_copy(j, half):
        return remote(
            rows_all.at[j, half], rows_all.at[j, half], pair_send.at[j], pair_recv.at[j],
            (z, f, other),
        )

    @pl.when(z < n_rep - 1)
    def _():
        row_copy(z, rows_up, z + 1).start()

    @pl.when(z > 0)
    def _():
        row_copy(z, rows_down, z - 1).start()

    for which in (GATE, UP, DOWN):
        for side in (0, 1):
            weight_copy(which, side).start()
    pair_copy(z, t).start()

    for s in range(1, max(n_rep, 4)):
        if s <= 3:
            pass_weights(s - 1)
        if s >= n_rep:
            continue

        @pl.when(z - s >= 0)
        def _():
            row_copy(z - s, rows_up, z).wait_recv()
            pair_copy(z - s, t).start()

            @pl.when(z < n_rep - 1)
            def _():
                row_copy(z - s, rows_up, z + 1).start()

        @pl.when(z + s < n_rep)
        def _():
            row_copy(z + s, rows_down, z).wait_recv()
            pair_copy(z + s, t).start()

            @pl.when(z > 0)
            def _():
                row_copy(z + s, rows_down, z - 1).start()

    for j in range(n_rep):
        pair_copy(j, other).wait_recv()
    for which in (GATE, UP, DOWN):
        for side in (0, 1):
            weight_across(which, side).wait_recv()

    def forward(j, carry):
        normed = rows_all[j, :, 0].reshape(chunk, width)
        cotangent = rows_all[j, :, 1].reshape(chunk, width)
        gate_pre = jnp.dot(
            normed, gate_all[...].reshape(width, hidden_units), preferred_element_type=jnp.float32
        )
        up_pre = jnp.dot(
            normed, up_all[...].reshape(width, hidden_units), preferred_element_type=jnp.float32
        )
        grad_hidden = jnp.zeros((chunk, hidden_units), jnp.float32)
        for k in range(n_fs):
            grad_hidden += contract_cols(cotangent[:, k * block : (k + 1) * block], down_all[k])
        grad_hidden = 0.5 * grad_hidden
        sigmoid_gate = jax.nn.sigmoid(gate_pre)
        activated = gate_pre * sigmoid_gate
        at = pl.ds(pl.multiple_of(j * chunk, chunk), chunk)
        hidden_all[at, :] = (activated * up_pre).astype(jnp.bfloat16)
        grad_up_pre = (grad_hidden * activated).astype(jnp.bfloat16)
        grad_gate_pre = (
            grad_hidden * up_pre * sigmoid_gate * (1.0 + gate_pre * (1.0 - sigmoid_gate))
        ).astype(jnp.bfloat16)
        grad_up[at, :] = grad_up_pre
        grad_gate[at, :] = grad_gate_pre
        return carry

    lax.fori_loop(0, n_rep, forward, 0)

    def backward(j, carry):
        at = pl.ds(pl.multiple_of(j * chunk, chunk), chunk)
        for k in range(n_fs):
            part = contract_cols(grad_gate[at, :], gate_all[k]) + contract_cols(
                grad_up[at, :], up_all[k]
            )
            normed_part[j, :, :, k * block : (k + 1) * block] = part.reshape(2, local, block)
        return carry

    def partner_copy(j):
        return remote(
            normed_part.at[j, other], partner_part.at[j], partner_ssem.at[j], partner_rsem.at[j],
            (z, f, other),
        )

    def columns_of(half, k):
        at = pl.ds(pl.multiple_of(k * block, block), block)
        return rows_all[:, :, half, :, at].reshape(n_rep * chunk, block)

    def term(which, k):
        if which == GATE:
            return contract_rows(grad_gate[...], columns_of(0, k))
        if which == UP:
            return contract_rows(grad_up[...], columns_of(0, k))
        return contract_rows(hidden_all[...], columns_of(1, k))

    sums = ((gate_send, gate_recv), (up_send, up_recv), (down_send, down_recv))

    def half(which, part):
        rows = sums[which][0].shape[1] // 2
        return pl.ds(part * rows, rows)

    def scatter_copy(which, side, kind):
        source, target = sums[which]
        at = half(which, side)
        slot = (1 + side) if kind == 0 else 3
        sem = 2 * side + kind
        return remote(
            source.at[slot, at], target.at[kind, at],
            scatter_ssem.at[which, sem], scatter_rsem.at[which, sem], (z, sides[side], t),
        )

    def pass_copy(which, side):
        source, target = sums[which]
        at = half(which, 1 - side)
        return remote(
            source.at[1 + side, at], target.at[2, at],
            scatter_ssem.at[which, 4 + side], scatter_rsem.at[which, 4 + side],
            (z, sides[side], t),
        )

    def send_terms(which):
        sums[which][0][3] = term(which, across)
        for side in (0, 1):
            scatter_copy(which, side, 1).start()
        for side in (0, 1):
            sums[which][0][1 + side] = term(which, sides[side])
            scatter_copy(which, side, 0).start()

    def pass_sums(which):
        source, target = sums[which]
        for side in (0, 1):
            scatter_copy(which, 1 - side, 1).wait_recv()
            at = half(which, 1 - side)
            source[1 + side, at] = source[1 + side, at] + target[1, at]
            pass_copy(which, side).start()

    def rep_copy(d):
        return remote(
            normed_part.at[shifted(z, d, n_rep), t], rep_part.at[d],
            rep_ssem.at[d], rep_rsem.at[d], (shifted(z, d, n_rep), f, t),
        )

    send_terms(GATE)
    lax.fori_loop(0, n_rep, backward, 0)
    for j in range(n_rep):
        partner_copy(j).start()
    send_terms(UP)
    for j in range(n_rep):
        partner_copy(j).wait_recv()
        normed_part[j, t] = normed_part[j, t] + partner_part[j]
    for d in range(1, n_rep):
        rep_copy(d).start()
    sums[GATE][0][0] = term(GATE, f)
    pass_sums(GATE)
    send_terms(DOWN)
    for which in (UP, DOWN):
        sums[which][0][0] = term(which, f)

    outs = ((gate_low, gate_high), (up_low, up_high), (down_low, down_high))

    class gather_copy:
        def __init__(self, which, j, sems, to):
            self.pieces = [
                remote(
                    out.at[j], out.at[j], sems.at[which, part, j],
                    gather_rsem.at[which, part, j], (to, f, t),
                )
                for part, out in enumerate(outs[which])
            ]

        def start(self):
            for piece in self.pieces:
                piece.start()

        def wait_recv(self):
            for piece in self.pieces:
                piece.wait_recv()

        def wait_send(self):
            for piece in self.pieces:
                piece.wait_send()

    def row_squares(value):
        return lax.dot_general(
            jnp.ones((8, value.shape[1]), jnp.float32), value * value,
            (((1,), (1,)), ((), ())), preferred_element_type=jnp.float32,
            precision=lax.Precision.HIGHEST,
        )

    def own_sum(which):
        source, target = sums[which]
        for side in (0, 1):
            scatter_copy(which, side, 0).wait_recv()
            pass_copy(which, side).wait_recv()
        total = source[0] + target[0] + target[2]
        total = total * (factor if which != DOWN else 0.5 * factor)
        cut = outs[which][0].shape[1]
        outs[which][0][z] = total[:cut].astype(jnp.bfloat16)
        outs[which][1][z] = total[cut:]

        @pl.when(z < n_rep - 1)
        def _():
            gather_copy(which, z, gather_up, z + 1).start()

        @pl.when(z > 0)
        def _():
            gather_copy(which, z, gather_down, z - 1).start()

        if which == DOWN:
            row_parts[z, f] = row_squares(total)
        else:
            squares = jnp.sum(total * total, axis=0, keepdims=True)
            column_parts[z, t, which] = jnp.broadcast_to(squares, (8, block))

    def relay(which, s):
        @pl.when((z - s >= 0) & (z < n_rep - 1))
        def _():
            gather_copy(which, z - s, gather_up, z).wait_recv()
            gather_copy(which, z - s, gather_up, z + 1).start()

        @pl.when((z + s < n_rep) & (z > 0))
        def _():
            gather_copy(which, z + s, gather_down, z).wait_recv()
            gather_copy(which, z + s, gather_down, z - 1).start()

    def collect(which, s):
        @pl.when((z - s >= 0) & (z == n_rep - 1))
        def _():
            gather_copy(which, z - s, gather_up, z).wait_recv()

        @pl.when((z + s < n_rep) & (z == 0))
        def _():
            gather_copy(which, z + s, gather_down, z).wait_recv()

    def column_copy(dz, dt):
        return remote(
            column_parts.at[z, t], column_parts.at[z, t],
            column_ssem.at[dz, dt], column_rsem.at[dz, dt],
            (shifted(z, dz, n_rep), f, shifted(t, dt, 2)),
        )

    def column_arrival(dz, dt):
        at_z, at_t = shifted(z, n_rep - dz, n_rep), shifted(t, dt, 2)
        return remote(
            column_parts.at[z, t], column_parts.at[at_z, at_t],
            column_ssem.at[dz, dt], column_rsem.at[dz, dt],
            (shifted(z, dz, n_rep), f, shifted(t, dt, 2)),
        )

    def row_power_copy(dz, df):
        return remote(
            row_parts.at[z, f], row_parts.at[z, f], row_ssem.at[dz, df], row_rsem.at[dz, df],
            (shifted(z, dz, n_rep), shifted(f, df, n_fs), t),
        )

    def row_power_arrival(dz, df):
        at_z, at_f = shifted(z, n_rep - dz, n_rep), shifted(f, n_fs - df, n_fs)
        return remote(
            row_parts.at[z, f], row_parts.at[at_z, at_f], row_ssem.at[dz, df],
            row_rsem.at[dz, df], (shifted(z, dz, n_rep), shifted(f, df, n_fs), t),
        )

    column_peers = [(dz, dt) for dz in range(n_rep) for dt in range(2) if dz or dt]
    row_peers = [(dz, df) for dz in range(n_rep) for df in range(n_fs) if dz or df]

    own_sum(GATE)
    pass_sums(UP)
    relay(GATE, 1)
    pass_sums(DOWN)
    own_sum(UP)
    for peer in column_peers:
        column_copy(*peer).start()
    for s in range(2, n_rep - 1):
        relay(GATE, s)
    own_sum(DOWN)
    for peer in row_peers:
        row_power_copy(*peer).start()
    for s in range(1, n_rep - 1):
        relay(UP, s)
    for s in range(1, n_rep - 1):
        relay(DOWN, s)

    grad_normed = normed_part[z, t]
    for d in range(1, n_rep):
        rep_copy(d).wait_recv()
        grad_normed = grad_normed + rep_part[d]
    normed_exact, recip_norm = normalise()
    inner = jnp.sum(grad_normed * normed_exact, axis=1, keepdims=True) * (1.0 / width)
    input_ref[...] = (recip_norm * (grad_normed - normed_exact * inner)).astype(jnp.bfloat16)

    for which in (GATE, UP, DOWN):
        for s in range(1, n_rep):
            collect(which, s)
    for peer in column_peers:
        column_arrival(*peer).wait_recv()
    for peer in row_peers:
        row_power_arrival(*peer).wait_recv()
    column_power[...] = jnp.sum(column_parts[...].reshape((2 * n_rep,) + column_parts.shape[2:]), axis=0)
    row_power[...] = jnp.sum(row_parts[...], axis=1)

    for which in (GATE, UP, DOWN):
        for side in (0, 1):
            weight_copy(which, side).wait_send()
            weight_forward(which, side).wait_send()
            scatter_copy(which, side, 0).wait_send()
            scatter_copy(which, side, 1).wait_send()
            pass_copy(which, side).wait_send()
    for j in range(n_rep):
        pair_copy(j, t).wait_send()
        partner_copy(j).wait_send()

        @pl.when((z < n_rep - 1) & (z >= j))
        def _():
            row_copy(j, rows_up, z).wait_send()
            for which in (GATE, UP, DOWN):
                gather_copy(which, j, gather_up, z).wait_send()

        @pl.when((z > 0) & (z <= j))
        def _():
            row_copy(j, rows_down, z).wait_send()
            for which in (GATE, UP, DOWN):
                gather_copy(which, j, gather_down, z).wait_send()
    for d in range(1, n_rep):
        rep_copy(d).wait_send()
    for peer in column_peers:
        column_copy(*peer).wait_send()
    for peer in row_peers:
        row_power_copy(*peer).wait_send()


def assemble_kernel(
    n_rep, width,
    gate_low, gate_high, up_low, up_high, down_low, down_high, column_power, row_power,
    gate_out, up_out, down_out, gate_power, up_power, down_power,
):
    cut = gate_low.shape[1]
    units = cut + gate_high.shape[1]
    for j in range(n_rep):
        at = slice(j * units, (j + 1) * units)
        for low, high, out in ((gate_low, gate_high, gate_out), (up_low, up_high, up_out)):
            both = jnp.concatenate([low[j].astype(jnp.float32), high[j]], axis=0)
            out[:, at] = both.T
        down_out[j * units : j * units + cut, :] = down_low[j].astype(jnp.float32)
        down_out[j * units + cut : (j + 1) * units, :] = down_high[j]
        down_power[:, at] = row_power[j, 0:1] * (1.0 / width)
    gate_power[...] = column_power[0, 0:1] * (1.0 / (2 * n_rep * units))
    up_power[...] = column_power[1, 0:1] * (1.0 / (2 * n_rep * units))


def on_device_fused(n_rep, n_fs, tokens, cotangent, gate_weight, up_weight, down_weight):
    local, width = tokens.shape
    block, hidden_local = gate_weight.shape
    units = hidden_local // n_rep
    factor = 1.0 / math.sqrt(local * 2 * n_rep * n_fs)
    count = n_rep * 2 * local
    cut = units * 13 // 16 // 16 * 16
    f32, bf16 = jnp.float32, jnp.bfloat16
    shapes = (
        jax.ShapeDtypeStruct((local, width), bf16),
        *[
            jax.ShapeDtypeStruct((n_rep, cut, block), bf16),
            jax.ShapeDtypeStruct((n_rep, units - cut, block), f32),
        ] * 3,
        jax.ShapeDtypeStruct((2, 8, block), f32),
        jax.ShapeDtypeStruct((n_rep, 8, units), f32),
    )
    dma = pltpu.SemaphoreType.DMA
    vmem = pltpu.VMEM
    scratch = [
        vmem((n_rep, 2, 2, local, width), bf16),
        vmem((n_fs, block, units), bf16),
        vmem((n_fs, block, units), bf16),
        vmem((n_fs, units, block), bf16),
        vmem((count, units), bf16),
        vmem((count, units), bf16),
        vmem((count, units), bf16),
        vmem((n_rep, 2, local, width), f32),
        vmem((n_rep, local, width), f32),
        vmem((n_rep, local, width), f32),
        *[vmem((n_fs, units, block), f32)] * 6,
        vmem((n_rep, 2, 2, 8, block), f32),
        vmem((n_rep, n_fs, 8, units), f32),
        dma((n_rep,)), dma((n_rep,)), dma((n_rep,)), dma((n_rep,)), dma((n_rep,)),
        dma((3, 4)), dma((3, 4)),
        dma((n_rep,)), dma((n_rep,)), dma((n_rep,)), dma((n_rep,)),
        dma((3, 6)), dma((3, 6)),
        dma((3, 2, n_rep)), dma((3, 2, n_rep)), dma((3, 2, n_rep)),
        dma((n_rep, 2)), dma((n_rep, 2)), dma((n_rep, n_fs)), dma((n_rep, n_fs)),
    ]
    whole = pl.BlockSpec(memory_space=pltpu.VMEM)
    input_grad, *blocks = pl.pallas_call(
        functools.partial(exchange_kernel, n_rep, n_fs, factor),
        out_shape=shapes,
        in_specs=[whole] * 5,
        out_specs=(whole,) * 9,
        scratch_shapes=scratch,
        compiler_params=pltpu.CompilerParams(
            collective_id=0, has_side_effects=True, vmem_limit_bytes=63 * 1024 * 1024
        ),
    )(tokens, cotangent, gate_weight, up_weight, down_weight)
    gate_grad, up_grad, down_grad, gate_power, up_power, down_power = pl.pallas_call(
        functools.partial(assemble_kernel, n_rep, width),
        out_shape=(
            jax.ShapeDtypeStruct((block, hidden_local), f32),
            jax.ShapeDtypeStruct((block, hidden_local), f32),
            jax.ShapeDtypeStruct((hidden_local, block), f32),
            jax.ShapeDtypeStruct((1, block), f32),
            jax.ShapeDtypeStruct((1, block), f32),
            jax.ShapeDtypeStruct((1, hidden_local), f32),
        ),
        in_specs=[whole] * 8,
        out_specs=(whole,) * 6,
        compiler_params=pltpu.CompilerParams(vmem_limit_bytes=63 * 1024 * 1024),
    )(*blocks)
    return (
        input_grad, gate_grad, up_grad, down_grad,
        gate_power.reshape(block), up_power.reshape(block), down_power.reshape(hidden_local),
    )


def solution(mesh):
    placed = (
        P(("rep", "fs", "tp"), None),
        P(("rep", "fs", "tp"), None),
        P("fs", "tp"),
        P("fs", "tp"),
        P("tp", "fs"),
    )
    n_rep, n_fs = mesh.shape["rep"], mesh.shape["fs"]

    def step(tokens, cotangent, gate_weight, up_weight, down_weight):
        block, hidden_local = gate_weight.shape
        run = on_device
        if mesh.shape["tp"] == 2 and n_fs == 4:
            if hidden_local % (16 * n_rep) == 0 and block % 128 == 0:
                run = functools.partial(on_device_fused, n_rep, n_fs)
        return run(tokens, cotangent, gate_weight, up_weight, down_weight)

    return jax.shard_map(
        step,
        mesh=mesh,
        in_specs=placed,
        out_specs=(
            P(("rep", "fs", "tp"), None),
            P("fs", "tp"),
            P("fs", "tp"),
            P("tp", "fs"),
            P("fs"),
            P("fs"),
            P("tp"),
        ),
        check_vma=False,
    )
```
